128 devices in a mesh: ep: 64 (over z, y, x), tp: 2 (over core).
Axes of the slice: x: 4, y: 4, z: 4, core: 2. Of those that a mesh axis runs over, the one named last changes fastest.
Arguments:
- tokens: bfloat16 [1024, 2048], P('ep'), may hold values from -6 to 6
- norm_attn: float32 [2048], replicated, may hold values from 0.1 to 1.9
- w_query: bfloat16 [2048, 2048], P(None, 'tp'), may hold values from -0.125 to 0.125
- w_key: bfloat16 [2048, 256], P(None, 'tp'), may hold values from -0.125 to 0.125
- w_value: bfloat16 [2048, 256], P(None, 'tp'), may hold values from -0.125 to 0.125
- w_out: bfloat16 [2048, 2048], P('tp'), may hold values from -0.125 to 0.125
- attn_bias: float32 [32], P('tp'), may hold values from -7 to -1
- cache_keys: bfloat16 [1024, 1024, 256], P('ep', None, 'tp'), may hold values from -6 to 6
- cache_values: bfloat16 [1024, 1024, 256], P('ep', None, 'tp'), may hold values from -6 to 6
- lengths: int32 [1024], P('ep'), may hold values from 256 to 1024
- norm_ffn: float32 [2048], replicated, may hold values from 0.1 to 1.9
- expert_gate: bfloat16 [2048, 57344], P(None, ('ep', 'tp')), may hold values from -0.125 to 0.125
- expert_up: bfloat16 [2048, 57344], P(None, ('ep', 'tp')), may hold values from -0.125 to 0.125
- expert_down: bfloat16 [57344, 2048], P(('ep', 'tp')), may hold values from -0.0625 to 0.0625
- dense_gate_w: bfloat16 [2048, 7168], P(None, 'ep'), may hold values from -0.125 to 0.125
- dense_up_w: bfloat16 [2048, 7168], P(None, 'ep'), may hold values from -0.125 to 0.125
- dense_down_w: bfloat16 [7168, 2048], P('ep'), may hold values from -0.0625 to 0.0625
- dense_mix: bfloat16 [2048], replicated, may hold values from -0.125 to 0.125
- routes: int32 [1024, 2], P(('ep', 'tp')), may hold values from 0 to 7, all different within a row; in each aligned block of 8 rows (0 to 7, 8 to 15, ...) at most 3 rows name the same one
- route_weights: bfloat16 [1024, 2], P(('ep', 'tp')), may hold values from 0.19921875 to 1
Outputs:
- layer_out: bfloat16 [1024, 2048], P(('ep', 'tp'))
- new_keys: bfloat16 [1024, 256], P('ep', 'tp')
- new_values: bfloat16 [1024, 256], P('ep', 'tp')
The draws below stay inside these ranges and needn't reach their ends.
Inputs may be any that keep to these rules, and one draw needn't show every extreme that they name: `routes`: in each aligned block of 8 rows (the rows of one device) no expert is named by more than 3 rows, a bound that some block reaches; a row names 2 different experts.
All inputs are finite; a program needn't handle non-finite values.
Results may differ from the reference program's by a relative error of at most 0.015.
Values may be sent and summed in bfloat16 or wider, within the bound.
A program may use at most 128 MiB of HBM per device.

```python
import math
import jax
import jax.numpy as jnp
import numpy as np
from jax import lax

D = 2048
HEADS = 32
KV_HEADS = 4
HEAD_DIM = 64
FF = 7168
DENSE_FF = 7168
EXPERTS = 8
TOP = 2
SEQS_DEV = 16
CACHE = 1024
TOKENS = 1024
ROWS_DEV = 8
CAP_DEV = 3
N_EP = 64
N_TP = 2


def place_ends(drawn, key, low, largest):
    dims = drawn.shape
    spot = [jax.random.randint(jax.random.fold_in(key, axis), (), 0, dims[axis]) for axis in range(len(dims))]
    drawn = drawn.at[tuple(spot)].set(low)
    longest = dims.index(max(dims))
    spot[longest] = (spot[longest] + 1) % dims[longest]
    return drawn.at[tuple(spot)].set(largest)


def steps_of(own_key, dims, pieces, smallest, top_value):
    def one(position, blocks):
        steps = jax.random.uniform(jax.random.fold_in(jax.random.fold_in(own_key, 6), position), (blocks,), jnp.float32, smallest / len(pieces), top_value / len(pieces))
        return jnp.repeat(jnp.exp(steps), dims[position] // blocks).reshape((-1,) + (1,) * (len(dims) - position - 1))

    level = one(*pieces[0])
    for cut in pieces[1:]:
        level = level * one(*cut)
    return level


def assign_block(key, own, number, rows, count, top, limit, lean):
    sequence = jax.random.permutation(key, count)
    crowded, ordinary = portions_of(count, rows * top, limit, lean, True), portions_of(count, rows * top, limit, lean, False)
    places = jnp.arange(count)

    def named(tallies, rotation):
        used = int((tallies > 0).sum())
        fixed = max(1, used // 4)
        moved = fixed + (places - fixed + rotation * (used - fixed)) % max(1, count - fixed)
        return jnp.zeros((count,), jnp.int32).at[sequence[jnp.where(places < fixed, places, moved)]].set(jnp.asarray(tallies, jnp.int32))

    tallies = jnp.where(number % 4 == 0, named(crowded, number // 4), named(ordinary, number - number // 4 - 1))
    mixed = jax.random.permutation(jax.random.fold_in(own, 3), count)
    source_of, sink = mixed[0:count // 2 * 2:2], mixed[1:count // 2 * 2:2]
    margin = jnp.minimum(tallies[source_of] - 1, limit - tallies[sink]) // 2
    margin = jnp.where((source_of == sequence[0]) | (sink == sequence[0]) | (tallies[sink] == 0), 0, jnp.maximum(margin, 0))
    moved = jax.random.randint(jax.random.fold_in(own, 4), (count // 2,), 0, 1 << 20) % (margin + 1)
    tallies = tallies.at[source_of].add(-moved).at[sink].add(moved)
    members = jnp.searchsorted(jnp.cumsum(tallies), jnp.arange(rows * top), side="right").astype(jnp.int32)
    grid = members.reshape(top, rows).T
    grid = grid[jax.random.permutation(jax.random.fold_in(own, 1), rows)]
    rotation = jax.random.randint(jax.random.fold_in(own, 2), (rows, 1), 0, top)
    return jnp.take_along_axis(grid, (jnp.arange(top)[None, :] + rotation) % top, axis=1)


def portions_of(amount, total, reach, slope, full):
    weights = [(1 << 20) // math.isqrt(grade ** slope) + 1 for grade in range(1, amount + 1)]
    largest = reach if full else min(reach, max(-(-total // amount), total * weights[0] // sum(weights)))
    least = 1 if total - largest >= amount - 1 else 0
    given, surplus = [largest] + [least] * (amount - 1), total - largest - least * (amount - 1)
    while surplus > 0:
        free = [i for i in range(1, amount) if given[i] < largest] or [i for i in range(1, amount) if given[i] < reach]
        whole, budget = sum([weights[i] for i in free]), surplus
        for i in free:
            extra = min(reach - given[i], max(1, budget * weights[i] // whole), surplus)
            given[i] = given[i] + extra
            surplus = surplus - extra
    return np.array(given)


def scatter_about(key, dims, deviation, bound, cuts=(), kind=jnp.bfloat16):
    drawn = deviation * jax.random.normal(key, dims, jnp.float32)
    if cuts:
        drawn = drawn * steps_of(key, dims, cuts, -0.22, 0.18)
    return jnp.clip(drawn, -bound, bound).astype(kind)


def setup_inputs(seed: int = 0) -> dict:
    key_of = jax.random.split(jax.random.key(seed), 21)
    tokens = scatter_about(key_of[0], (TOKENS, D), 1.0, 6.0, ((0, 64),))
    norm_attn = jnp.clip(1.0 + 0.18 * jax.random.normal(key_of[1], (D,), jnp.float32), 0.1, 1.9)
    w_query = scatter_about(key_of[2], (D, HEADS * HEAD_DIM), D ** -0.5, 0.125, ((1, 2),))
    w_key = scatter_about(key_of[3], (D, KV_HEADS * HEAD_DIM), D ** -0.5, 0.125, ((1, 2),))
    w_value = scatter_about(key_of[4], (D, KV_HEADS * HEAD_DIM), D ** -0.5, 0.125, ((1, 2),))
    w_out = scatter_about(key_of[5], (HEADS * HEAD_DIM, D), (HEADS * HEAD_DIM) ** -0.5, 0.125, ((0, 2),))
    attn_bias = jnp.clip(-7.0 + 6.0 * jax.random.uniform(key_of[6], (HEADS,), jnp.float32) ** steps_of(key_of[6], (HEADS,), ((0, 2),), -0.2, 0.2), -7.0, -1.0)
    cache_keys = scatter_about(key_of[7], (TOKENS, CACHE, KV_HEADS * HEAD_DIM), 1.0, 6.0, ((0, 64), (2, 2)))
    cache_values = scatter_about(key_of[8], (TOKENS, CACHE, KV_HEADS * HEAD_DIM), 1.0, 6.0, ((0, 64), (2, 2)))
    lengths = place_ends(jax.random.randint(key_of[9], (TOKENS,), CACHE // 4, CACHE + 1), jax.random.fold_in(key_of[9], 1), CACHE // 4, CACHE).astype(jnp.int32)
    norm_ffn = jnp.clip(1.0 + 0.18 * jax.random.normal(key_of[10], (D,), jnp.float32), 0.1, 1.9)
    expert_gate = scatter_about(key_of[11], (D, EXPERTS * FF), D ** -0.5, 0.125, ((1, 128),))
    expert_up = scatter_about(key_of[12], (D, EXPERTS * FF), D ** -0.5, 0.125, ((1, 128),))
    expert_down = scatter_about(key_of[13], (EXPERTS * FF, D), FF ** -0.5, 0.0625, ((0, 128),))
    dense_gate_w = scatter_about(key_of[14], (D, DENSE_FF), D ** -0.5, 0.125, ((1, 64),))
    dense_up_w = scatter_about(key_of[15], (D, DENSE_FF), D ** -0.5, 0.125, ((1, 64),))
    dense_down_w = scatter_about(key_of[16], (DENSE_FF, D), DENSE_FF ** -0.5, 0.0625, ((0, 64),))
    dense_mix = scatter_about(key_of[17], (D,), D ** -0.5, 0.125)
    routes_keys = jax.random.split(jax.random.fold_in(key_of[18], 1), TOKENS // ROWS_DEV)
    routes_turns = jax.random.permutation(jax.random.fold_in(key_of[18], 3), TOKENS // ROWS_DEV)
    routes = jax.vmap(lambda own, number: assign_block(jax.random.fold_in(key_of[18], 2), own, number, ROWS_DEV, EXPERTS, TOP, CAP_DEV, 1))(routes_keys, routes_turns).reshape((TOKENS, TOP))
    route_weights = jnp.clip(jnp.exp(math.log(1.0) - 1.6133518 * jax.random.uniform(key_of[19], (TOKENS, TOP), jnp.float32) ** steps_of(key_of[19], (TOKENS, TOP), ((0, 128),), -0.2, 0.2)), 0.19921875, 1.0).astype(jnp.bfloat16)
    return {"tokens": tokens, "norm_attn": norm_attn, "w_query": w_query, "w_key": w_key, "w_value": w_value, "w_out": w_out, "attn_bias": attn_bias, "cache_keys": cache_keys, "cache_values": cache_values, "lengths": lengths, "norm_ffn": norm_ffn, "expert_gate": expert_gate, "expert_up": expert_up, "expert_down": expert_down, "dense_gate_w": dense_gate_w, "dense_up_w": dense_up_w, "dense_down_w": dense_down_w, "dense_mix": dense_mix, "routes": routes, "route_weights": route_weights}


EPSILON = 1e-06

def normed_rows(values, gain):
    widened = values.astype(jnp.float32)
    scale = lax.rsqrt(lax.optimization_barrier(jnp.mean(widened * widened, axis=-1, keepdims=True)) + EPSILON)
    return (widened * scale * gain).astype(jnp.bfloat16)

def reference(tokens, norm_attn, w_query, w_key, w_value, w_out, attn_bias, cache_keys, cache_values, lengths, norm_ffn, expert_gate, expert_up, expert_down, dense_gate_w, dense_up_w, dense_down_w, dense_mix, routes, route_weights):
    repeat = HEADS // KV_HEADS
    normed = normed_rows(tokens, norm_attn)
    query = jnp.dot(normed, w_query, preferred_element_type=jnp.float32).astype(jnp.bfloat16)
    new_keys = jnp.dot(normed, w_key, preferred_element_type=jnp.float32).astype(jnp.bfloat16)
    new_values = jnp.dot(normed, w_value, preferred_element_type=jnp.float32).astype(jnp.bfloat16)
    offsets = attn_bias.reshape(KV_HEADS, repeat)

    def attend(block):
        query_block, key_block, value_block, length_block = block
        query_heads = query_block.astype(jnp.float32).reshape(SEQS_DEV, KV_HEADS, repeat, HEAD_DIM)
        key_heads = key_block.astype(jnp.float32).reshape(SEQS_DEV, CACHE, KV_HEADS, HEAD_DIM)
        value_heads = value_block.astype(jnp.float32).reshape(SEQS_DEV, CACHE, KV_HEADS, HEAD_DIM)
        scores = jnp.einsum('bgrd,bsgd->bgrs', query_heads, key_heads) * HEAD_DIM ** (-0.5)
        scores = scores + offsets[None, :, :, None]
        places = lax.broadcasted_iota(jnp.int32, (SEQS_DEV, CACHE), 1)
        visible = (places < length_block[:, None])[:, None, None, :]
        log_keep = jnp.where(visible, jax.nn.log_sigmoid(-scores), 0.0)
        after = lax.cumsum(log_keep, axis=3, reverse=True) - log_keep
        weight = jnp.where(visible, jnp.exp(jax.nn.log_sigmoid(scores) + after), 0.0).astype(jnp.bfloat16)
        mixed = jnp.einsum('bgrs,bsgd->bgrd', weight.astype(jnp.float32), value_heads)
        return mixed.astype(jnp.bfloat16).reshape(SEQS_DEV, HEADS * HEAD_DIM)
    heads_out = lax.map(attend, (query.reshape(N_EP, SEQS_DEV, HEADS * HEAD_DIM), cache_keys.reshape(N_EP, SEQS_DEV, CACHE, KV_HEADS * HEAD_DIM), cache_values.reshape(N_EP, SEQS_DEV, CACHE, KV_HEADS * HEAD_DIM), lengths.reshape(N_EP, SEQS_DEV))).reshape(TOKENS, HEADS * HEAD_DIM)
    run_width = HEADS * HEAD_DIM // N_TP
    attn_sum = jnp.zeros((TOKENS, D), jnp.float32)
    for run in range(N_TP):
        partial_value = jnp.dot(heads_out[:, run * run_width:(run + 1) * run_width], w_out[run * run_width:(run + 1) * run_width], preferred_element_type=jnp.float32)
        attn_sum = attn_sum + lax.optimization_barrier(partial_value.astype(jnp.bfloat16)).astype(jnp.float32)
    middle = (tokens.astype(jnp.float32) + attn_sum).astype(jnp.bfloat16)
    normed_two = normed_rows(middle, norm_ffn)
    mix_gate = jax.nn.sigmoid(jnp.dot(normed_two, dense_mix, preferred_element_type=jnp.float32))
    dense_hidden = (jax.nn.silu(jnp.dot(normed_two, dense_gate_w, preferred_element_type=jnp.float32)) * jnp.dot(normed_two, dense_up_w, preferred_element_type=jnp.float32)).astype(jnp.bfloat16)
    dense_term = jnp.dot(dense_hidden, dense_down_w, preferred_element_type=jnp.float32) * mix_gate[:, None]
    sources = N_EP * N_TP
    route_blocks = routes.reshape(sources, ROWS_DEV, TOP)
    weight_blocks = route_weights.astype(jnp.float32).reshape(sources, ROWS_DEV, TOP)
    row_blocks = normed_two.astype(jnp.float32).reshape(sources, ROWS_DEV, D)
    slot_ids = lax.broadcasted_iota(jnp.int32, (sources, CAP_DEV, ROWS_DEV), 1)

    def one_expert(expert_id):
        matched = route_blocks == expert_id
        present = jnp.any(matched, axis=2).astype(jnp.int32)
        share = lax.optimization_barrier(jnp.sum(jnp.where(matched, weight_blocks, 0.0), axis=2))
        ranks = jnp.cumsum(present, axis=1) - 1
        selector = ((present[:, None, :] == 1) & (ranks[:, None, :] == slot_ids)).astype(jnp.float32)
        slot_rows = jnp.einsum('dcr,drk->dck', selector, row_blocks).astype(jnp.bfloat16).reshape(sources * CAP_DEV, D)
        start = (expert_id * FF).astype(jnp.int32)
        gate_cols = lax.dynamic_slice_in_dim(expert_gate, start, FF, 1)
        up_cols = lax.dynamic_slice_in_dim(expert_up, start, FF, 1)
        down_rows = lax.dynamic_slice_in_dim(expert_down, start, FF, 0)
        hidden = (jax.nn.silu(jnp.dot(slot_rows, gate_cols, preferred_element_type=jnp.float32)) * jnp.dot(slot_rows, up_cols, preferred_element_type=jnp.float32)).astype(jnp.bfloat16)
        result = jnp.dot(hidden, down_rows, preferred_element_type=jnp.float32).reshape(sources, CAP_DEV, D)
        returned = jnp.einsum('dcr,dck->drk', selector, result) * share[:, :, None]
        return returned.reshape(TOKENS, D)
    expert_term = lax.optimization_barrier(jnp.sum(lax.map(one_expert, jnp.arange(EXPERTS, dtype=jnp.int32)), axis=0))
    layer_out = (middle.astype(jnp.float32) + expert_term + dense_term).astype(jnp.bfloat16)
    return (layer_out, new_keys, new_values)
```

```python
import functools
import jax
import jax.numpy as jnp
from jax import lax
from jax.experimental import pallas as pl
from jax.experimental.pallas import tpu as pltpu
from jax.sharding import PartitionSpec as P

D = 2048
BF = jnp.bfloat16
F32 = jnp.float32
EPSILON = 1e-06
SEQS = 16
CACHE = 1024
HEADS = 16
NT = (((1,), (1,)), ((), ()))
VM = pl.BlockSpec(memory_space=pltpu.VMEM)
HB = pl.BlockSpec(memory_space=pl.ANY)


def normed_rows(widened, gain):
    scale = lax.rsqrt(jnp.mean(widened * widened, axis=-1, keepdims=True) + EPSILON)
    return (widened * scale * gain).astype(BF)


def column_of(row, count):
    rows = lax.broadcasted_iota(jnp.int32, (count, count), 0)
    cols = lax.broadcasted_iota(jnp.int32, (count, count), 1)
    wide = jnp.broadcast_to(row, (count, count))
    return jnp.sum(jnp.where(rows == cols, wide, 0.0), axis=1, keepdims=True)


def attention_kernel(
    tokens, norm, bias, lengths, wq_h, wk_h, wv_h, wo_h, ck_h, cv_h,
    part, nk, nv,
    wq, wk, wv, wo, ck, cv, qs, xs, sq, sw, so, sk, sv,
):
    def q_copy(i):
        rows = pl.ds(i * 512, 512)
        return pltpu.make_async_copy(wq_h.at[rows], wq.at[rows], sq.at[i])

    def o_copy(i):
        place = (i % 8) * 128 + (i // 8) * 64
        return pltpu.make_async_copy(wo_h.at[pl.ds(i * 64, 64)], wo.at[pl.ds(place, 64)], so.at[i])

    def k_copy(b):
        return pltpu.make_async_copy(ck_h.at[b], ck.at[b], sk.at[b])

    def v_copy(b):
        return pltpu.make_async_copy(cv_h.at[b], cv.at[b], sv.at[b])

    wk_copy = pltpu.make_async_copy(wk_h, wk, sw.at[0])
    wv_copy = pltpu.make_async_copy(wv_h, wv, sw.at[1])
    for i in range(4):
        q_copy(i).start()
    for b in range(SEQS):
        k_copy(b).start()
        v_copy(b).start()
    for i in range(16):
        o_copy(i).start()
    wk_copy.start()
    wv_copy.start()

    normed = normed_rows(tokens[...].astype(F32), norm[...])
    query = jnp.zeros((SEQS, HEADS * 64), F32)
    for i in range(4):
        q_copy(i).wait()
        query += jnp.dot(normed[:, i * 512 : (i + 1) * 512], wq[pl.ds(i * 512, 512), :], preferred_element_type=F32)
    query = query.astype(BF).astype(F32) * 0.125
    lane = lax.broadcasted_iota(jnp.int32, (SEQS, 128), 1)
    for i in range(8):
        pair = query[:, i * 128 : (i + 1) * 128]
        turned = pltpu.roll(pair, 64, 1)
        for j in range(2):
            h = 2 * i + j
            low = h < 8
            chosen = pair if (j == 0) == low else turned
            keep = (lane < 64) if low else (lane >= 64)
            qs[:, h, :] = jnp.where(keep, chosen, 0.0)

    bias_col = column_of(bias[...], HEADS)
    tri = (
        lax.broadcasted_iota(jnp.int32, (256, 256), 0) > lax.broadcasted_iota(jnp.int32, (256, 256), 1)
    ).astype(BF)
    places = lax.broadcasted_iota(jnp.int32, (HEADS, CACHE), 1)
    lane8 = lax.broadcasted_iota(jnp.int32, (8, 128), 1)

    def one_sequence(b):
        k_copy(b).wait()
        z = lax.dot_general(qs[b].astype(BF), ck[b], NT, preferred_element_type=F32) + bias_col
        visible = places < lengths[b]
        tail = jnp.log(1.0 + jnp.exp(-jnp.abs(z)))
        log_take = jnp.minimum(z, 0.0) - tail
        log_keep = jnp.where(visible, jnp.minimum(-z, 0.0) - tail, 0.0)
        high = log_keep.astype(BF)
        rest = (log_keep - high.astype(F32)).astype(BF)
        blocks = [high[:, n * 256 : (n + 1) * 256] for n in range(4)]
        blocks += [rest[:, n * 256 : (n + 1) * 256] for n in range(4)]
        sums = jnp.dot(jnp.concatenate(blocks, axis=0), tri, preferred_element_type=F32)
        later = jnp.zeros((HEADS, 1), F32)
        after = [None] * 4
        for n in range(3, -1, -1):
            inner = sums[n * 16 : (n + 1) * 16] + sums[64 + n * 16 : 64 + (n + 1) * 16]
            after[n] = inner + later
            later = later + inner[:, 0:1] + log_keep[:, n * 256 : n * 256 + 1]
        weight = jnp.where(visible, jnp.exp(log_take + jnp.concatenate(after, axis=1)), 0.0).astype(BF)
        v_copy(b).wait()
        mixed = jnp.dot(weight, cv[b], preferred_element_type=F32)
        xs[b] = jnp.where(lane8 < 64, mixed[0:8], mixed[8:16])

    def some(i, carry):
        for j in range(4):
            one_sequence(i * 4 + j)
        return carry

    lax.fori_loop(0, SEQS // 4, some, 0)

    for i in range(16):
        o_copy(i).wait()
    heads = jnp.concatenate([xs[:, r, :].astype(BF) for r in range(8)], axis=1)
    part[...] = jnp.dot(heads, wo[...], preferred_element_type=F32).astype(BF)
    wk_copy.wait()
    wv_copy.wait()
    nk[...] = jnp.dot(normed, wk[...], preferred_element_type=F32).astype(BF)
    nv[...] = jnp.dot(normed, wv[...], preferred_element_type=F32).astype(BF)


def attention(tokens, norm, bias, lengths, wq, wk, wv, wo, ck, cv):
    return pl.pallas_call(
        attention_kernel,
        out_shape=(
            jax.ShapeDtypeStruct((SEQS, D), BF),
            jax.ShapeDtypeStruct((SEQS, 128), BF),
            jax.ShapeDtypeStruct((SEQS, 128), BF),
        ),
        in_specs=[VM, VM, VM, pl.BlockSpec(memory_space=pltpu.SMEM)] + [HB] * 6,
        out_specs=(VM, VM, VM),
        scratch_shapes=[
            pltpu.VMEM((D, 1024), BF),
            pltpu.VMEM((D, 128), BF),
            pltpu.VMEM((D, 128), BF),
            pltpu.VMEM((1024, D), BF),
            pltpu.VMEM((SEQS, CACHE, 128), BF),
            pltpu.VMEM((SEQS, CACHE, 128), BF),
            pltpu.VMEM((SEQS, HEADS, 128), F32),
            pltpu.VMEM((SEQS, 8, 128), F32),
            pltpu.SemaphoreType.DMA((4,)),
            pltpu.SemaphoreType.DMA((2,)),
            pltpu.SemaphoreType.DMA((16,)),
            pltpu.SemaphoreType.DMA((SEQS,)),
            pltpu.SemaphoreType.DMA((SEQS,)),
        ],
        compiler_params=pltpu.CompilerParams(vmem_limit_bytes=40 * 1024 * 1024),
        name="attention",
    )(tokens, norm.reshape(1, D), bias.reshape(1, HEADS), lengths, wq, wk, wv, wo, ck, cv)


EXPERTS = 8
TOP = 2


def split_up(shard, dim, count):
    dims = shard.shape
    pieces = shard.reshape(*dims[:dim], count, dims[dim] // count, *dims[dim + 1 :])
    return jnp.moveaxis(pieces, dim, 0)


def sum_at_owner(shard, axis, dim):
    pieces = split_up(shard, dim, lax.axis_size(axis))
    arrived = lax.all_to_all(pieces, axis, split_axis=0, concat_axis=0, tiled=True)
    return arrived.astype(jnp.float32).sum(axis=0)


def sent_to_all(shard, axis):
    copies = jnp.broadcast_to(shard, (lax.axis_size(axis), *shard.shape))
    return lax.all_to_all(copies, axis, split_axis=0, concat_axis=0, tiled=True)


def joined_along(pieces, dim):
    pieces = jnp.moveaxis(pieces, 0, dim)
    dims = pieces.shape
    return pieces.reshape(*dims[:dim], dims[dim] * dims[dim + 1], *dims[dim + 2 :])


def gather_directly(shard, axis, dim):
    pieces = sent_to_all(shard, axis)
    return joined_along(pieces, dim)


def running_ranks(present):
    count = present.shape[-1]
    rows_in = lax.broadcasted_iota(jnp.int32, (count, count), 0)
    cols_in = lax.broadcasted_iota(jnp.int32, (count, count), 1)
    lower = (rows_in <= cols_in).astype(jnp.float32)
    totals = jnp.einsum(
        "...j,ji->...i", present.astype(jnp.float32), lower, precision=lax.Precision.HIGHEST
    )
    return totals.astype(jnp.int32) - 1


def shards(
    tokens,
    norm_attn,
    w_query,
    w_key,
    w_value,
    w_out,
    attn_bias,
    cache_keys,
    cache_values,
    lengths,
    norm_ffn,
    expert_gate,
    expert_up,
    expert_down,
    dense_gate_w,
    dense_up_w,
    dense_down_w,
    dense_mix,
    routes,
    route_weights,
):
    seq_count = tokens.shape[0]
    partial_value, new_keys, new_values = attention(
        tokens, norm_attn, attn_bias, lengths, w_query, w_key, w_value, w_out, cache_keys, cache_values
    )
    attn_sum = sum_at_owner(partial_value, "tp", 0)
    row_count = seq_count // lax.axis_size("tp")
    capacity = (row_count * TOP + EXPERTS - 1) // EXPERTS + 1
    own_rows = lax.dynamic_slice_in_dim(tokens, lax.axis_index("tp") * row_count, row_count, 0)
    middle = (own_rows.astype(jnp.float32) + attn_sum).astype(jnp.bfloat16)
    normed_two = normed_rows(middle.astype(F32), norm_ffn)
    width = normed_two.shape[1]
    piece = gather_directly(normed_two, "ep", 0)
    mix_gate = jax.nn.sigmoid(jnp.dot(piece, dense_mix, preferred_element_type=jnp.float32))
    dense_hidden = (
        jax.nn.silu(jnp.dot(piece, dense_gate_w, preferred_element_type=jnp.float32))
        * jnp.dot(piece, dense_up_w, preferred_element_type=jnp.float32)
    ).astype(jnp.bfloat16)
    dense_terms = (
        jnp.dot(dense_hidden, dense_down_w, preferred_element_type=jnp.float32) * mix_gate[:, None]
    )
    dense_term = sum_at_owner(dense_terms.astype(jnp.bfloat16), "ep", 0)
    devices = lax.axis_size(("ep", "tp"))
    members = devices // EXPERTS
    expert_ids = lax.broadcasted_iota(jnp.int32, (EXPERTS, 1, 1), 0)
    matched = routes[None, :, :] == expert_ids
    present = jnp.any(matched, axis=2).astype(jnp.int32)
    share = jnp.sum(jnp.where(matched, route_weights.astype(jnp.float32)[None, :, :], 0.0), axis=2)
    ranks = running_ranks(present)
    slot_ids = lax.broadcasted_iota(jnp.int32, (EXPERTS, capacity, row_count), 1)
    selector = (present[:, None, :] == 1) & (ranks[:, None, :] == slot_ids)
    slot_rows = jnp.einsum(
        "ecr,rk->eck", selector.astype(jnp.bfloat16), normed_two, preferred_element_type=jnp.float32
    ).astype(jnp.bfloat16)
    outgoing = jnp.repeat(slot_rows, members, axis=0)
    incoming = lax.all_to_all(outgoing, ("ep", "tp"), split_axis=0, concat_axis=0, tiled=True)
    slot_rows = incoming.reshape(devices * capacity, width)
    expert_hidden = (
        jax.nn.silu(jnp.dot(slot_rows, expert_gate, preferred_element_type=jnp.float32))
        * jnp.dot(slot_rows, expert_up, preferred_element_type=jnp.float32)
    ).astype(jnp.bfloat16)
    expert_result = jnp.dot(expert_hidden, expert_down, preferred_element_type=jnp.float32).reshape(
        devices, capacity, width
    )
    back = lax.all_to_all(
        expert_result.astype(jnp.bfloat16), ("ep", "tp"), split_axis=0, concat_axis=0, tiled=True
    ).astype(expert_result.dtype)
    per_expert = jnp.sum(back.reshape(EXPERTS, members, capacity, width), axis=1)
    expert_term = jnp.einsum("ecr,eck,er->rk", selector.astype(jnp.float32), per_expert, share)
    layer_out = (middle.astype(jnp.float32) + expert_term + dense_term).astype(jnp.bfloat16)
    return (layer_out, new_keys, new_values)


def solution(mesh):
    placed = (
        P("ep", None),
        P(),
        P(None, "tp"),
        P(None, "tp"),
        P(None, "tp"),
        P("tp", None),
        P("tp"),
        P("ep", None, "tp"),
        P("ep", None, "tp"),
        P("ep"),
        P(),
        P(None, ("ep", "tp")),
        P(None, ("ep", "tp")),
        P(("ep", "tp"), None),
        P(None, "ep"),
        P(None, "ep"),
        P("ep", None),
        P(),
        P(("ep", "tp"), None),
        P(("ep", "tp"), None),
    )
    return jax.shard_map(
        shards,
        mesh=mesh,
        in_specs=placed,
        out_specs=(P(("ep", "tp"), None), P("ep", "tp"), P("ep", "tp")),
        check_vma=False,
    )
```

```python
import functools
import jax
import jax.numpy as jnp
from jax import lax
from jax.experimental import pallas as pl
from jax.experimental.pallas import tpu as pltpu
from jax.sharding import PartitionSpec as P

D = 2048
BF = jnp.bfloat16
F32 = jnp.float32
EPSILON = 1e-06
SEQS = 16
CACHE = 1024
HEADS = 16
NT = (((1,), (1,)), ((), ()))
VM = pl.BlockSpec(memory_space=pltpu.VMEM)
HB = pl.BlockSpec(memory_space=pltpu.HBM)


def normed_rows(widened, gain):
    scale = lax.rsqrt(jnp.mean(widened * widened, axis=-1, keepdims=True) + EPSILON)
    return (widened * scale * gain).astype(BF)


def column_of(row, count):
    rows = lax.broadcasted_iota(jnp.int32, (count, count), 0)
    cols = lax.broadcasted_iota(jnp.int32, (count, count), 1)
    wide = jnp.broadcast_to(row, (count, count))
    return jnp.sum(jnp.where(rows == cols, wide, 0.0), axis=1, keepdims=True)


HALF = D // 2
WIDE = HALF + 128
MESH = pl.DeviceIdType.MESH
GATHER = (((0, 384), (2, 1, 0)), ((384, 384), (1, 0, 2)), ((768, 384), (0, 2, 1)))
SCATTER = (((0, 384), (0, 1, 2)), ((384, 384), (2, 0, 1)), ((768, 256), (1, 2, 0)))
HIDDEN = 512
GROUP = 4
N_RECV = 102
PHASE = [None]


def phase(name):
    if PHASE[0] is not None:
        PHASE[0].__exit__(None, None, None)
    PHASE[0] = jax.named_scope(name) if name else None
    if name:
        PHASE[0].__enter__()


def layer_kernel(
    tokens, norm, bias, lengths, gain, mix_w, routes, route_w,
    wq_h, wk_h, wv_h, wo_h, ck_h, cv_h, eg_h, eu_h, ed_h, dg_h, du_h, dd_h,
    out, nk, nv,
    wq, wk, wv, wo, ckv, qs, xs, part,
    rx, mid, gath, weights, hid, ps, pin, tot, rb, fin, t1, r2, res, got,
    sq, skv, so, sw, wsem, psem, gsem, csem, rsem,
):
    phase("start")
    ep = lax.axis_index("ep")
    core = lax.axis_index("tp")
    other = 1 - core
    me = (ep // 16, lax.rem(ep // 4, 4), lax.rem(ep, 4))
    strides = (16, 4, 1)

    def shifted(axis, k):
        return lax.rem(me[axis] + (k + 4), 4)

    def chip_at(axis, k, second=0, m=0):
        far = ep + (shifted(axis, k) - me[axis]) * strides[axis]
        return far + (shifted(second, m) - me[second]) * strides[second], core

    peer = (ep, other)
    barrier = pltpu.get_barrier_semaphore()
    pl.semaphore_signal(barrier, inc=1, device_id=peer, device_id_type=MESH)
    for axis in range(3):
        for k in range(1, 4):
            pl.semaphore_signal(barrier, inc=1, device_id=chip_at(axis, k), device_id_type=MESH)
            for m in range(1, 4):
                target = chip_at(axis, k, (axis + 1) % 3, m)
                pl.semaphore_signal(barrier, inc=1, device_id=target, device_id_type=MESH)

    def q_copy(i):
        rows = pl.ds(i * 512, 512)
        return pltpu.make_async_copy(wq_h.at[rows], wq.at[rows], sq.at[i])

    def cache_start(i):
        rows = pl.ds(i * GROUP, GROUP)
        pltpu.make_async_copy(ck_h.at[rows], ckv.at[0, rows], skv.at[i]).start()
        pltpu.make_async_copy(cv_h.at[rows], ckv.at[1, rows], skv.at[i]).start()

    def cache_wait(i):
        both = ckv.at[:, pl.ds(i * GROUP, GROUP)]
        pltpu.make_async_copy(both, both, skv.at[i]).wait()

    ck, cv = ckv.at[0], ckv.at[1]
    wk_copy = pltpu.make_async_copy(wk_h, wk, sw.at[0])
    wv_copy = pltpu.make_async_copy(wv_h, wv, sw.at[1])
    for i in range(4):
        q_copy(i).start()
    cache_start(0)

    kind = lax.broadcasted_iota(jnp.int32, (8, 128), 1)
    meta = jnp.zeros((8, 128), F32)
    for k in range(2):
        chosen = column_of(routes[k : k + 1, :].astype(F32), 8).astype(jnp.int32)
        share = column_of(route_w[k : k + 1, :].astype(F32), 8)
        meta += jnp.where(kind == chosen, share, 0.0)
    part[core, :, D : D + 128] = meta.astype(BF)
    part[other, :, D : D + 128] = jnp.zeros((8, 128), BF)

    normed_all = normed_rows(jnp.concatenate([tokens[0].astype(F32), tokens[1].astype(F32)], axis=0), norm[...])
    phase("query")
    query = jnp.zeros((SEQS, HEADS * 64), F32)
    for i in range(4):
        q_copy(i).wait()
        if i < 3:
            cache_start(i + 1)
        query += jnp.dot(normed_all[:, i * 512 : (i + 1) * 512], wq[pl.ds(i * 512, 512), :], preferred_element_type=F32)
    for i in range(16):
        row = (i % 8) * 128 + (i // 8) * 64
        pltpu.make_async_copy(wo_h.at[pl.ds(i * 64, 64)], wo.at[pl.ds(row, 64)], so).start()
    wk_copy.start()
    wv_copy.start()
    query = query.astype(BF).astype(F32) * 0.125
    lane = lax.broadcasted_iota(jnp.int32, (SEQS, 128), 1)
    for i in range(8):
        pair = query[:, i * 128 : (i + 1) * 128]
        turned = pltpu.roll(pair, 64, 1)
        for j in range(2):
            h = 2 * i + j
            low = h < 8
            chosen = pair if (j == 0) == low else turned
            keep = (lane < 64) if low else (lane >= 64)
            qs[:, h, :] = jnp.where(keep, chosen, 0.0)

    phase("attend")
    bias_col = column_of(bias[...], HEADS)
    tri = (
        lax.broadcasted_iota(jnp.int32, (256, 256), 0) > lax.broadcasted_iota(jnp.int32, (256, 256), 1)
    ).astype(BF)
    places = lax.broadcasted_iota(jnp.int32, (HEADS, CACHE), 1)
    lane8 = lax.broadcasted_iota(jnp.int32, (8, 128), 1)

    def some(i, carry):
        group = [i * GROUP + j for j in range(GROUP)]
        cache_wait(i)
        scores = [
            lax.dot_general(qs[b].astype(BF), ck[b], NT, preferred_element_type=F32) + bias_col for b in group
        ]
        takes, keeps, seen, stacked = [], [], [], []
        for b, z in zip(group, scores):
            visible = places < lengths[b]
            tail = jnp.log(1.0 + jnp.exp(-jnp.abs(z)))
            log_take = jnp.minimum(z, 0.0) - tail
            log_keep = jnp.where(visible, log_take - z, 0.0)
            high = log_keep.astype(BF)
            rest = (log_keep - high.astype(F32)).astype(BF)
            takes.append(log_take)
            keeps.append(log_keep)
            seen.append(visible)
            for n in range(4):
                stacked.append(high[:, n * 256 : (n + 1) * 256])
                stacked.append(rest[:, n * 256 : (n + 1) * 256])
        sums = jnp.dot(jnp.concatenate(stacked, axis=0), tri, preferred_element_type=F32)
        weights = []
        for at in range(GROUP):
            later = jnp.zeros((HEADS, 1), F32)
            after = [None] * 4
            for n in range(3, -1, -1):
                row = at * 128 + n * 32
                inner = sums[row : row + 16] + sums[row + 16 : row + 32]
                after[n] = inner + later
                later = later + inner[:, 0:1] + keeps[at][:, n * 256 : n * 256 + 1]
            after = jnp.concatenate(after, axis=1)
            weights.append(jnp.where(seen[at], jnp.exp(takes[at] + after), 0.0).astype(BF))
        for b, weight in zip(group, weights):
            mixed = jnp.dot(weight, cv[b], preferred_element_type=F32)
            xs[b] = jnp.where(lane8 < 64, mixed[0:8], mixed[8:16])
        return carry

    lax.fori_loop(0, SEQS // GROUP, some, 0)

    phase("project")
    base = pl.multiple_of(core * 48, 16)
    loads = (
        (eg_h, 0, 448), (dg_h.at[pl.ds(base, 64)], 448, 64),
        (eu_h, 512, 448), (du_h.at[pl.ds(base, 64)], 960, 64),
        (ed_h, 1024, 448), (dd_h.at[pl.ds(base, 64)], 1472, 64),
    )
    for src, row, count in loads:
        pltpu.make_async_copy(src, weights.at[pl.ds(row, count)], wsem).start()
    pltpu.make_async_copy(wo, wo, so).wait()
    heads = jnp.concatenate([xs[:, r, :].astype(BF) for r in range(8)], axis=1)
    value = jnp.dot(heads, wo[...], preferred_element_type=F32)
    part[0, :, 0:D] = value[0:8].astype(BF)
    part[1, :, 0:D] = value[8:16].astype(BF)

    used = [0]

    def slots(count):
        used[0] += count
        return list(range(used[0] - count, used[0]))

    def send(src, dst, device, sem, slot):
        pltpu.make_async_remote_copy(
            src_ref=src, dst_ref=dst, send_sem=sem, recv_sem=rsem.at[slot], device_id=device, device_id_type=MESH
        ).start()

    def arrived(ref, slot):
        pltpu.make_async_remote_copy(
            src_ref=ref, dst_ref=ref, send_sem=csem, recv_sem=rsem.at[slot], device_id=peer, device_id_type=MESH
        ).wait_recv()

    pl.semaphore_wait(barrier, 37)
    phase("pair")
    (slot,) = slots(1)
    send(part, rx, peer, psem, slot)
    wk_copy.wait()
    wv_copy.wait()
    nk[...] = jnp.dot(normed_all, wk[...], preferred_element_type=F32).astype(BF)
    nv[...] = jnp.dot(normed_all, wv[...], preferred_element_type=F32).astype(BF)
    arrived(rx, slot)
    phase("norm")
    mix_row = mix_w[...].astype(F32).reshape(1, D)
    for h in range(2):
        summed = part[h].astype(F32) + rx[h].astype(F32)
        middle = (tokens[h].astype(F32) + summed[:, 0:D]).astype(BF).astype(F32)
        normed = normed_rows(middle, gain[...]).astype(F32)
        mix = jax.nn.sigmoid(jnp.sum(normed * mix_row, axis=1, keepdims=True))
        mix_high = mix.astype(BF).astype(F32)
        meta = jnp.where(kind == 8, mix_high, summed[:, D : D + 128])
        meta = jnp.where(kind == 9, mix - mix_high, meta)
        mid[h] = jnp.where(core == 0, middle[:, 0:HALF], middle[:, HALF:D])
        own = jnp.where(core == 0, normed[:, 0:HALF], normed[:, HALF:D])
        gath[h, core, me[0], me[1], me[2], :, 0:HALF] = own.astype(BF)
        gath[h, core, me[0], me[1], me[2], :, HALF:WIDE] = meta.astype(BF)

    whole = pl.ds(0, 4)
    parts = range(3)
    steps = (1, -1, 2)
    upward, downward = (0, 2), (1, -1)
    g2 = gath.reshape(2, 2, 512, WIDE)

    def sized(rows, lanes):
        return g2.at[0, 0, pl.ds(0, rows), pl.ds(lanes[0], lanes[1])]

    class Gather:
        def __init__(self, h):
            self.h = h
            self.first = slots(3)
            self.second = [dict(zip(steps, slots(3))) for p in parts]
            self.below = [dict(zip((0, 2, 1), slots(3))) for p in parts]
            self.above = [dict(zip((1, -1, 0), slots(3))) for p in parts]
            for p in parts:
                self.below[p][-1] = self.below[p][1]
                self.above[p][2] = self.above[p][0]
            self.relayed = slots(3)
            (self.across,) = slots(1)

        def held(self, lanes, where):
            at = [me[0], me[1], me[2]]
            for axis, index in where.items():
                at[axis] = index
            return gath.at[self.h, core, at[0], at[1], at[2], :, pl.ds(lanes[0], lanes[1])]

        def spread(self, block, device, slot):
            send(block, block, device, gsem, slot)

        def plane(self):
            for m in (0, *steps):
                for k in (0, *steps):
                    for p, (lanes, (a, b, c)) in enumerate(GATHER):
                        if (k, m) != (0, 0):
                            slot = self.second[p][m] if m else self.first[p]
                            self.spread(self.held(lanes, {}), chip_at(a, k, b, m), slot)

        def bulk(self, p, o):
            lanes, (a, b, c) = GATHER[p]
            if o:
                arrived(sized(32, lanes), self.second[p][-o if o != 2 else 2])
            else:
                arrived(sized(24, lanes), self.first[p])
            block = self.held(lanes, {a: whole, b: shifted(b, o)})
            self.spread(block, chip_at(c, 1), self.below[p][o])
            self.spread(block, chip_at(c, -1), self.above[p][o])

        def rounds(self):
            for o in (0, *steps):
                for p in parts:
                    self.bulk(p, o)
            for p in parts:
                self.hand_over(p, 0)

        def hand_over(self, p, o):
            lanes, (a, b, c) = GATHER[p]
            self.spread(self.held(lanes, {a: whole, b: whole, c: shifted(c, o)}), peer, self.across)

        def relay(self, o):
            for p, (lanes, (a, b, c)) in enumerate(GATHER):
                below = o in upward
                arrived(sized(32, lanes), (self.below if below else self.above)[p][o])
                block = self.held(lanes, {a: whole, b: shifted(b, o), c: shifted(c, -1 if below else 1)})
                self.spread(block, chip_at(c, 1 if below else -1), self.relayed[p])

        def neighbours(self):
            for p, (lanes, _) in enumerate(GATHER):
                arrived(sized(64, lanes), self.below[p][1])
                self.hand_over(p, -1)
                arrived(sized(64, lanes), self.above[p][0])
                self.hand_over(p, 1)

        def farthest(self):
            for p, (lanes, _) in enumerate(GATHER):
                arrived(sized(128, lanes), self.relayed[p])
                self.hand_over(p, 2)

        def complete(self):
            arrived(g2.at[self.h, 0], self.across)

    expert = ep // 8
    column = lax.broadcasted_iota(jnp.int32, (1, 256), 1) + 256
    dense_own = jnp.logical_and(column >= 448, jnp.logical_or(core == 0, column >= 464))
    kinds = lax.broadcasted_iota(jnp.int32, (256, 128), 1)

    def hidden_unit(h, i, n):
        rows = slice(i * 256, (i + 1) * 256)
        x = [g2[h, c, rows, 0:HALF] for c in range(2)]
        info = g2[h, 0, rows, HALF:WIDE].astype(F32)
        factor = jnp.sum(jnp.where(kinds == expert, info, 0.0), axis=1, keepdims=True)
        if n == 1:
            mixed = info[:, 8:9] + info[:, 9:10]
            factor = jnp.where(column < 448, factor, jnp.where(dense_own, mixed, 0.0))

        def product(row):
            w = weights[row : row + 256, :]
            y = lax.dot_general(x[0], w[:, 0:HALF], NT, preferred_element_type=F32)
            return y + lax.dot_general(x[1], w[:, HALF:D], NT, preferred_element_type=F32)

        g = product(n * 256)
        u = product(HIDDEN + n * 256)
        hid[h, rows, n * 256 : (n + 1) * 256] = g * jax.nn.sigmoid(g) * u * factor

    h4 = hid.reshape(2, 4, 4, 4, 8, HIDDEN)
    halves = (pl.ds(0, 2), pl.ds(2, 2))

    def place(axis, index):
        at = [slice(None)] * 3
        at[axis] = index
        return tuple(at)

    def summand(ref, lanes, axis, where, half=None):
        at = [whole, whole, whole]
        at[axis] = where
        if half is not None:
            at[1 if axis == 0 else 0] = half
        return ref.at[at[0], at[1], at[2], :, pl.ds(lanes[0], lanes[1])]

    def cells(axis, index):
        for i in range(4):
            for j in range(4):
                at = [i, j]
                at.insert(axis, index)
                yield i, j, tuple(at)

    offsets = [(m, k) for m in (2, 1, -1, 0) for k in (2, 1, -1, 0) if (m, k) != (0, 0)]

    class Scatter:
        def __init__(self, h):
            self.h = h
            self.swap = dict(zip((2, 1, -1, 0), slots(4)))
            self.far = [slots(2) for p in parts]
            self.last = slots(3)
            self.nexts = slots(3)

        def down(self, o):
            h = self.h
            for p, (lanes, (a, b, c)) in enumerate(SCATTER):
                cut = slice(lanes[0], lanes[0] + lanes[1])
                high = slice(HALF + lanes[0], HALF + lanes[0] + lanes[1])
                rows = place(a, shifted(a, o))
                x = h4[(h,) + rows + (slice(None), slice(None))].reshape(128, HIDDEN).astype(BF)
                w = jnp.concatenate([weights[2 * HIDDEN :, cut], weights[2 * HIDDEN :, high]], axis=1)
                y = jnp.dot(x, w, preferred_element_type=F32)
                for half in range(2):
                    piece = y[:, half * lanes[1] : (half + 1) * lanes[1]].reshape(4, 4, 8, lanes[1])
                    ps[(h, half) + rows + (slice(None), cut)] = piece.astype(BF)
                send(
                    summand(ps.at[h, other], lanes, a, shifted(a, o)), summand(pin.at[h], lanes, a, shifted(a, o)),
                    peer, csem, self.swap[o],
                )

        def joined(self, p, o):
            h = self.h
            lanes, (a, b, c) = SCATTER[p]
            cut = slice(lanes[0], lanes[0] + lanes[1])
            if p == 0:
                arrived(pin.at[h, 0], self.swap[o])
            for i, j, at in cells(a, shifted(a, o)):
                at = at + (slice(None), cut)
                tot[(h,) + at] = (ps[(h, core) + at].astype(F32) + pin[(h,) + at].astype(F32)).astype(BF)

        def open(self):
            h = self.h
            for p, (lanes, (a, b, c)) in enumerate(SCATTER):
                self.joined(p, 2)
                for way, k in enumerate((1, -1)):
                    send(
                        summand(tot.at[h], lanes, a, shifted(a, 2), halves[way]),
                        rb.at[h, way, :, :, :, pl.ds(lanes[0], lanes[1])],
                        chip_at(a, k), csem, self.far[p][way],
                    )

        def near(self, k):
            h = self.h
            way = 0 if k == 1 else 1
            half = halves[1 - way]
            for p, (lanes, (a, b, c)) in enumerate(SCATTER):
                self.joined(p, k)
                send(
                    summand(tot.at[h], lanes, a, shifted(a, k), half),
                    fin.at[h, way, half, :, :, pl.ds(lanes[0], lanes[1])],
                    chip_at(a, k), csem, self.last[p],
                )

        def close(self):
            h = self.h
            for p, (lanes, (a, b, c)) in enumerate(SCATTER):
                cut = slice(lanes[0], lanes[0] + lanes[1])
                lanes_ds = pl.ds(lanes[0], lanes[1])
                for way, k in enumerate((1, -1)):
                    arrived(rb.at[h, way, :, :, :, lanes_ds], self.far[p][way])
                    for i, j, at in cells(a, shifted(a, k)):
                        if i // 2 == way:
                            at = (h,) + at + (slice(None), cut)
                            tot[at] = (tot[at].astype(F32) + rb[h, way, i % 2, j, :, cut].astype(F32)).astype(BF)
                    send(
                        summand(tot.at[h], lanes, a, shifted(a, k), halves[way]),
                        fin.at[h, way, halves[way], :, :, lanes_ds],
                        chip_at(a, k), csem, self.last[p],
                    )

        def own(self):
            for p in parts:
                self.joined(p, 0)

        def plane(self):
            h = self.h
            for p, (lanes, (a, b, c)) in enumerate(SCATTER):
                cut = slice(lanes[0], lanes[0] + lanes[1])
                lanes_ds = pl.ds(lanes[0], lanes[1])
                arrived(fin.at[h, :, :, :, :, lanes_ds], self.last[p])
                for i, j, at in cells(a, me[a]):
                    t1[h, i, j, :, cut] = (
                        tot[(h,) + at + (slice(None), cut)].astype(F32)
                        + fin[h, 0, i, j, :, cut].astype(F32)
                        + fin[h, 1, i, j, :, cut].astype(F32)
                    ).astype(BF)
                d, e = [axis for axis in range(3) if axis != a]
                for n, (m, k) in enumerate(offsets):
                    send(
                        t1.at[h, shifted(d, m), shifted(e, k), :, lanes_ds], r2.at[h, n, :, lanes_ds],
                        chip_at(d, m, e, k), csem, self.nexts[p],
                    )

        def total(self):
            h = self.h
            for p, (lanes, (a, b, c)) in enumerate(SCATTER):
                cut = slice(lanes[0], lanes[0] + lanes[1])
                arrived(r2.at[h, :, :, pl.ds(lanes[0], lanes[1])], self.nexts[p])
                d, e = [axis for axis in range(3) if axis != a]
                sum_ = mid[h, :, cut] + t1[h, me[d], me[e], :, cut].astype(F32)
                for n in range(15):
                    sum_ += r2[h, n, :, cut].astype(F32)
                res[h, :, cut] = sum_.astype(BF)

    phase("gather1")
    ga, gb = Gather(0), Gather(1)
    sa, sb = Scatter(0), Scatter(1)
    ga.plane()
    gb.plane()
    phase("gather2")
    ga.rounds()
    phase("gather3")
    ga.relay(0)
    gb.rounds()
    phase("gather4")
    for o in steps:
        ga.relay(o)
    gb.relay(0)
    ga.neighbours()
    phase("gather5")
    for o in steps:
        gb.relay(o)
    ga.farthest()
    pltpu.make_async_copy(weights, weights, wsem).wait()
    ga.complete()
    phase("hidden_a")
    hidden_unit(0, 0, 0)
    hidden_unit(0, 0, 1)
    gb.neighbours()
    hidden_unit(0, 1, 0)
    hidden_unit(0, 1, 1)
    phase("down_a")
    sa.down(2)
    gb.farthest()
    sa.down(1)
    sa.open()
    sa.down(-1)
    sa.near(1)
    sa.down(0)
    sa.near(-1)
    phase("complete_b")
    gb.complete()
    phase("hidden_b")
    hidden_unit(1, 0, 0)
    sa.own()
    hidden_unit(1, 0, 1)
    sa.close()
    hidden_unit(1, 1, 0)
    hidden_unit(1, 1, 1)
    phase("down_b")
    sb.down(2)
    sb.down(1)
    sb.open()
    phase("plane_a")
    sa.plane()
    phase("near_b")
    sb.down(-1)
    sb.near(1)
    sb.down(0)
    sb.near(-1)
    phase("close_b")
    sb.close()
    sb.own()
    phase("total_a")
    sa.total()
    phase("plane_b")
    sb.plane()
    phase("total_b")
    sb.total()
    phase("exchange")
    (slot,) = slots(1)
    send(res.at[other], got, peer, csem, slot)
    out[core] = res[core]
    arrived(got, slot)
    out[other] = got[...]
    phase("finish")
    assert used[0] == N_RECV, used[0]
    rows = gath.reshape(2048, WIDE).at[pl.ds(0, 2032)]
    pltpu.make_async_copy(rows, rows, gsem).wait()
    rows = ps.reshape(2048, HALF).at[pl.ds(0, 2040)]
    pltpu.make_async_copy(rows, rows, csem).wait()
    pltpu.make_async_copy(part, part, psem).wait()
    phase(None)


def finish_kernel(a, b, c, out, nk, nv):
    out[:, 0:HALF] = a[0]
    out[:, HALF:D] = a[1]
    nk[...] = b[...]
    nv[...] = c[...]


OUT_SHAPES = (
    jax.ShapeDtypeStruct((8, D), BF),
    jax.ShapeDtypeStruct((SEQS, 128), BF),
    jax.ShapeDtypeStruct((SEQS, 128), BF),
)


def layer(*args):
    return pl.pallas_call(
        layer_kernel,
        out_shape=(jax.ShapeDtypeStruct((2, 8, HALF), BF),) + OUT_SHAPES[1:],
        in_specs=[VM] * 3 + [pl.BlockSpec(memory_space=pltpu.SMEM)] + [VM] * 4 + [HB] * 12,
        out_specs=(VM, VM, VM),
        scratch_shapes=[
            pltpu.VMEM((D, 1024), BF),
            pltpu.VMEM((D, 128), BF),
            pltpu.VMEM((D, 128), BF),
            pltpu.VMEM((1024, D), BF),
            pltpu.VMEM((2, SEQS, CACHE, 128), BF),
            pltpu.VMEM((SEQS, HEADS, 128), F32),
            pltpu.VMEM((SEQS, 8, 128), F32),
            pltpu.VMEM((2, 8, D + 128), BF),
            pltpu.VMEM((2, 8, D + 128), BF),
            pltpu.VMEM((2, 8, HALF), F32),
            pltpu.VMEM((2, 2, 4, 4, 4, 8, WIDE), BF),
            pltpu.VMEM((3 * HIDDEN, D), BF),
            pltpu.VMEM((2, 512, HIDDEN), F32),
            pltpu.VMEM((2, 2, 4, 4, 4, 8, HALF), BF),
            pltpu.VMEM((2, 4, 4, 4, 8, HALF), BF),
            pltpu.VMEM((2, 4, 4, 4, 8, HALF), BF),
            pltpu.VMEM((2, 2, 2, 4, 8, HALF), BF),
            pltpu.VMEM((2, 2, 4, 4, 8, HALF), BF),
            pltpu.VMEM((2, 4, 4, 8, HALF), BF),
            pltpu.VMEM((2, 15, 8, HALF), BF),
            pltpu.VMEM((2, 8, HALF), BF),
            pltpu.VMEM((8, HALF), BF),
            pltpu.SemaphoreType.DMA((4,)),
            pltpu.SemaphoreType.DMA((4,)),
            pltpu.SemaphoreType.DMA,
            pltpu.SemaphoreType.DMA((2,)),
            pltpu.SemaphoreType.DMA,
            pltpu.SemaphoreType.DMA,
            pltpu.SemaphoreType.DMA,
            pltpu.SemaphoreType.DMA,
            pltpu.SemaphoreType.DMA((N_RECV,)),
        ],
        compiler_params=pltpu.CompilerParams(
            vmem_limit_bytes=63 * 1024 * 1024, collective_id=0, has_side_effects=True
        ),
        name="layer",
    )(*args)


def shards(
    tokens, norm_attn, w_query, w_key, w_value, w_out, attn_bias, cache_keys, cache_values, lengths,
    norm_ffn, expert_gate, expert_up, expert_down, dense_gate_w, dense_up_w, dense_down_w, dense_mix,
    routes, route_weights,
):
    results = layer(
        tokens.reshape(2, 8, D), norm_attn.reshape(1, D), attn_bias.reshape(1, HEADS), lengths,
        norm_ffn.reshape(1, D), dense_mix, routes.T, route_weights.T,
        w_query, w_key, w_value, w_out, cache_keys, cache_values,
        expert_gate.T, expert_up.T, expert_down, dense_gate_w.T, dense_up_w.T, dense_down_w,
    )
    return pl.pallas_call(
        finish_kernel, out_shape=OUT_SHAPES, in_specs=[VM] * 3, out_specs=(VM, VM, VM), name="finish"
    )(*results)


def solution(mesh):
    placed = (
        P("ep", None),
        P(),
        P(None, "tp"),
        P(None, "tp"),
        P(None, "tp"),
        P("tp", None),
        P("tp"),
        P("ep", None, "tp"),
        P("ep", None, "tp"),
        P("ep"),
        P(),
        P(None, ("ep", "tp")),
        P(None, ("ep", "tp")),
        P(("ep", "tp"), None),
        P(None, "ep"),
        P(None, "ep"),
        P("ep", None),
        P(),
        P(("ep", "tp"), None),
        P(("ep", "tp"), None),
    )
    return jax.shard_map(
        shards,
        mesh=mesh,
        in_specs=placed,
        out_specs=(P(("ep", "tp"), None), P("ep", "tp"), P("ep", "tp")),
        check_vma=False,
    )
```

```python
import functools
import jax
import jax.numpy as jnp
from jax import lax
from jax.experimental import pallas as pl
from jax.experimental.pallas import tpu as pltpu
from jax.sharding import PartitionSpec as P

D = 2048
BF = jnp.bfloat16
F32 = jnp.float32
EPSILON = 1e-06
SEQS = 16
CACHE = 1024
HEADS = 16
NT = (((1,), (1,)), ((), ()))
VM = pl.BlockSpec(memory_space=pltpu.VMEM)
HB = pl.BlockSpec(memory_space=pltpu.HBM)


def normed_rows(widened, gain):
    scale = lax.rsqrt(jnp.mean(widened * widened, axis=-1, keepdims=True) + EPSILON)
    return (widened * scale * gain).astype(BF)


def column_of(row, count):
    rows = lax.broadcasted_iota(jnp.int32, (count, count), 0)
    cols = lax.broadcasted_iota(jnp.int32, (count, count), 1)
    wide = jnp.broadcast_to(row, (count, count))
    return jnp.sum(jnp.where(rows == cols, wide, 0.0), axis=1, keepdims=True)


HALF = D // 2
WIDE = HALF + 128
MESH = pl.DeviceIdType.MESH
GATHER = (((0, 384), (2, 1, 0)), ((384, 384), (1, 0, 2)), ((768, 384), (0, 2, 1)))
SCATTER = (((0, 384), (0, 1, 2)), ((384, 384), (2, 0, 1)), ((768, 256), (1, 2, 0)))
HIDDEN = 512
GROUP = 4
DIRECT = (True, True, True, True)
N_RECV = 99 - 12 * sum(DIRECT[0:2]) - 6 * sum(DIRECT[2:4])
PHASE = [None]


def phase(name):
    if PHASE[0] is not None:
        PHASE[0].__exit__(None, None, None)
    PHASE[0] = jax.named_scope(name) if name else None
    if name:
        PHASE[0].__enter__()


def layer_kernel(
    tokens_h, norm_h, bias_h, lengths_h, gain_h, mix_h, routes_h, route_w_h,
    wq_h, wk_h, wv_h, wo_h, ck_h, cv_h, eg_h, eu_h, ed_h, dg_h, du_h, dd_h,
    out, nk, nv,
    tokens, norm, bias, lengths, gain, mix_w, routes, route_w, small,
    wq, wk, wv, wo, ckv, qs, xs, part,
    rx, mid, gath, weights, hid, ps, own_sum, pin, tot, rb, fin, t1, r2, res, got,
    sq, skv, so, sw, wsem, psem, gsem, csem, rsem,
):
    phase("start")
    ep = lax.axis_index("ep")
    core = lax.axis_index("tp")
    other = 1 - core
    me = (ep // 16, lax.rem(ep // 4, 4), lax.rem(ep, 4))
    strides = (16, 4, 1)

    def shifted(axis, k):
        return lax.rem(me[axis] + (k + 4), 4)

    def chip_at(axis, k, second=0, m=0):
        far = ep + (shifted(axis, k) - me[axis]) * strides[axis]
        return far + (shifted(second, m) - me[second]) * strides[second], core

    def q_copy(i):
        rows = pl.ds(i * 512, 512)
        return pltpu.make_async_copy(wq_h.at[rows], wq.at[rows], sq.at[i])

    def cache_start(i):
        rows = pl.ds(i * GROUP, GROUP)
        pltpu.make_async_copy(ck_h.at[rows], ckv.at[0, rows], skv.at[i]).start()
        pltpu.make_async_copy(cv_h.at[rows], ckv.at[1, rows], skv.at[i]).start()

    def cache_wait(i):
        both = ckv.at[:, pl.ds(i * GROUP, GROUP)]
        pltpu.make_async_copy(both, both, skv.at[i]).wait()

    ck, cv = ckv.at[0], ckv.at[1]
    wk_copy = pltpu.make_async_copy(wk_h, wk, sw.at[0])
    wv_copy = pltpu.make_async_copy(wv_h, wv, sw.at[1])
    def output_start():
        for i in range(16):
            row = (i % 8) * 128 + (i // 8) * 64
            pltpu.make_async_copy(wo_h.at[pl.ds(i * 64, 64)], wo.at[pl.ds(row, 64)], so).start()

    littles = [
        pltpu.make_async_copy(src, dst, small.at[n])
        for n, (src, dst) in enumerate((
            (tokens_h, tokens), (norm_h, norm), (routes_h, routes), (route_w_h, route_w),
            (bias_h, bias), (lengths_h, lengths), (gain_h, gain), (mix_h, mix_w),
        ))
    ]
    for copy in littles[:4]:
        copy.start()
    for i in range(4):
        q_copy(i).start()
    for copy in littles[4:]:
        copy.start()
    cache_start(0)
    peer = (ep, other)
    barrier = pltpu.get_barrier_semaphore()
    pl.semaphore_signal(barrier, inc=1, device_id=peer, device_id_type=MESH)
    for axis in range(3):
        for k in range(1, 4):
            pl.semaphore_signal(barrier, inc=1, device_id=chip_at(axis, k), device_id_type=MESH)
            for m in range(1, 4):
                target = chip_at(axis, k, (axis + 1) % 3, m)
                pl.semaphore_signal(barrier, inc=1, device_id=target, device_id_type=MESH)

    for copy in littles[:4]:
        copy.wait()

    kind = lax.broadcasted_iota(jnp.int32, (8, 128), 1)
    meta = jnp.zeros((8, 128), F32)
    for k in range(2):
        chosen = column_of(routes[k : k + 1, :].astype(F32), 8).astype(jnp.int32)
        share = column_of(route_w[k : k + 1, :].astype(F32), 8)
        meta += jnp.where(kind == chosen, share, 0.0)
    part[core, :, D : D + 128] = meta.astype(BF)
    part[other, :, D : D + 128] = jnp.zeros((8, 128), BF)

    normed_all = normed_rows(jnp.concatenate([tokens[0].astype(F32), tokens[1].astype(F32)], axis=0), norm[...])
    phase("query")
    query = jnp.zeros((SEQS, HEADS * 64), F32)
    for i in range(4):
        q_copy(i).wait()
        if i == 1:
            output_start()
        else:
            cache_start((1, 0, 2, 3)[i])
        query += jnp.dot(normed_all[:, i * 512 : (i + 1) * 512], wq[pl.ds(i * 512, 512), :], preferred_element_type=F32)
    wk_copy.start()
    wv_copy.start()
    query = query.astype(BF).astype(F32) * 0.125
    lane = lax.broadcasted_iota(jnp.int32, (SEQS, 128), 1)
    for i in range(8):
        pair = query[:, i * 128 : (i + 1) * 128]
        turned = pltpu.roll(pair, 64, 1)
        for j in range(2):
            h = 2 * i + j
            low = h < 8
            chosen = pair if (j == 0) == low else turned
            keep = (lane < 64) if low else (lane >= 64)
            qs[:, h, :] = jnp.where(keep, chosen, 0.0)

    phase("attend")
    for copy in littles[4:]:
        copy.wait()
    bias_col = column_of(bias[...], HEADS)
    tri = (
        lax.broadcasted_iota(jnp.int32, (256, 256), 0) > lax.broadcasted_iota(jnp.int32, (256, 256), 1)
    ).astype(BF)
    places = lax.broadcasted_iota(jnp.int32, (HEADS, CACHE), 1)
    lane8 = lax.broadcasted_iota(jnp.int32, (8, 128), 1)

    def attend(i):
        group = [i * GROUP + j for j in range(GROUP)]
        cache_wait(i)
        scores = [
            lax.dot_general(qs[b].astype(BF), ck[b], NT, preferred_element_type=F32) + bias_col for b in group
        ]
        takes, keeps, seen, stacked = [], [], [], []
        for b, z in zip(group, scores):
            visible = places < lengths[b]
            tail = jnp.log(1.0 + jnp.exp(-jnp.abs(z)))
            log_take = jnp.minimum(z, 0.0) - tail
            log_keep = jnp.where(visible, log_take - z, 0.0)
            high = log_keep.astype(BF)
            rest = (log_keep - high.astype(F32)).astype(BF)
            takes.append(log_take)
            keeps.append(log_keep)
            seen.append(visible)
            for n in range(4):
                stacked.append(high[:, n * 256 : (n + 1) * 256])
                stacked.append(rest[:, n * 256 : (n + 1) * 256])
        sums = jnp.dot(jnp.concatenate(stacked, axis=0), tri, preferred_element_type=F32)
        weights = []
        for at in range(GROUP):
            later = jnp.zeros((HEADS, 1), F32)
            after = [None] * 4
            for n in range(3, -1, -1):
                row = at * 128 + n * 32
                inner = sums[row : row + 16] + sums[row + 16 : row + 32]
                after[n] = inner + later
                later = later + inner[:, 0:1] + keeps[at][:, n * 256 : n * 256 + 1]
            after = jnp.concatenate(after, axis=1)
            weights.append(jnp.where(seen[at], jnp.exp(takes[at] + after), 0.0).astype(BF))
        for b, weight in zip(group, weights):
            mixed = jnp.dot(weight, cv[b], preferred_element_type=F32)
            xs[b] = jnp.where(lane8 < 64, mixed[0:8], mixed[8:16])

    def project(h):
        heads = jnp.concatenate([xs[h * 8 : (h + 1) * 8, r, :].astype(BF) for r in range(8)], axis=1)
        part[h, :, 0:D] = jnp.dot(heads, wo[...], preferred_element_type=F32).astype(BF)

    used = [0]

    def slots(count):
        used[0] += count
        return list(range(used[0] - count, used[0]))

    def send(src, dst, device, sem, slot):
        pltpu.make_async_remote_copy(
            src_ref=src, dst_ref=dst, send_sem=sem, recv_sem=rsem.at[slot], device_id=device, device_id_type=MESH
        ).start()

    def arrived(ref, slot):
        pltpu.make_async_remote_copy(
            src_ref=ref, dst_ref=ref, send_sem=csem, recv_sem=rsem.at[slot], device_id=peer, device_id_type=MESH
        ).wait_recv()

    pair_slots = slots(2)
    mix_row = mix_w[...].astype(F32).reshape(1, D)

    def pair(h):
        send(part.at[h], rx.at[h], peer, psem, pair_slots[h])

    def norm_half(h):
        arrived(rx.at[h], pair_slots[h])
        summed = part[h].astype(F32) + rx[h].astype(F32)
        middle = (tokens[h].astype(F32) + summed[:, 0:D]).astype(BF).astype(F32)
        normed = normed_rows(middle, gain[...]).astype(F32)
        mix = jax.nn.sigmoid(jnp.sum(normed * mix_row, axis=1, keepdims=True))
        mix_high = mix.astype(BF).astype(F32)
        meta = jnp.where(kind == 8, mix_high, summed[:, D : D + 128])
        meta = jnp.where(kind == 9, mix - mix_high, meta)
        mid[h] = jnp.where(core == 0, middle[:, 0:HALF], middle[:, HALF:D])
        own = jnp.where(core == 0, normed[:, 0:HALF], normed[:, HALF:D])
        gath[h, core, me[0], me[1], me[2], :, 0:HALF] = own.astype(BF)
        gath[h, core, me[0], me[1], me[2], :, HALF:WIDE] = meta.astype(BF)

    whole = pl.ds(0, 4)
    parts = range(3)
    steps = (1, -1, 2)
    upward, downward = (0, 2), (1, -1)
    g2 = gath.reshape(2, 2, 512, WIDE)

    def sized(rows, lanes):
        return g2.at[0, 0, pl.ds(0, rows), pl.ds(lanes[0], lanes[1])]

    class Gather:
        def __init__(self, h, direct):
            self.h, self.direct = h, direct
            self.first = slots(3)
            self.second = [dict(zip(steps, slots(3))) for p in parts]
            (self.across,) = slots(1)
            if direct:
                self.straight = [dict(zip(steps, slots(3))) for p in parts]
                return
            self.below = [dict(zip((0, 2, 1), slots(3))) for p in parts]
            self.above = [dict(zip((1, -1, 0), slots(3))) for p in parts]
            for p in parts:
                self.below[p][-1] = self.below[p][1]
                self.above[p][2] = self.above[p][0]
            self.relayed = slots(3)

        def held(self, lanes, where):
            at = [me[0], me[1], me[2]]
            for axis, index in where.items():
                at[axis] = index
            return gath.at[self.h, core, at[0], at[1], at[2], :, pl.ds(lanes[0], lanes[1])]

        def spread(self, block, device, slot):
            send(block, block, device, gsem, slot)

        def plane(self):
            for m in (0, *steps):
                for k in (0, *steps):
                    for p, (lanes, (a, b, c)) in enumerate(GATHER):
                        if (k, m) != (0, 0):
                            slot = self.second[p][m] if m else self.first[p]
                            self.spread(self.held(lanes, {}), chip_at(a, k, b, m), slot)

        def bulk(self, p, o):
            lanes, (a, b, c) = GATHER[p]
            if o:
                arrived(sized(32, lanes), self.second[p][-o if o != 2 else 2])
            else:
                arrived(sized(24, lanes), self.first[p])
            block = self.held(lanes, {a: whole, b: shifted(b, o)})
            if self.direct:
                for k in (2, 1, -1):
                    self.spread(block, chip_at(c, k), self.straight[p][k])
                return
            self.spread(block, chip_at(c, 1), self.below[p][o])
            self.spread(block, chip_at(c, -1), self.above[p][o])

        def rounds(self):
            for o in (0, *steps):
                for p in parts:
                    self.bulk(p, o)
            for p in parts:
                self.hand_over(p, 0)

        def hand_over(self, p, o):
            lanes, (a, b, c) = GATHER[p]
            self.spread(self.held(lanes, {a: whole, b: whole, c: shifted(c, o)}), peer, self.across)

        def relay(self, o):
            for p, (lanes, (a, b, c)) in enumerate(GATHER):
                below = o in upward
                arrived(sized(32, lanes), (self.below if below else self.above)[p][o])
                block = self.held(lanes, {a: whole, b: shifted(b, o), c: shifted(c, -1 if below else 1)})
                self.spread(block, chip_at(c, 1 if below else -1), self.relayed[p])

        def neighbours(self):
            if self.direct:
                for p, (lanes, _) in enumerate(GATHER):
                    for k in (1, -1):
                        arrived(sized(128, lanes), self.straight[p][k])
                        self.hand_over(p, -k)
                return
            for p, (lanes, _) in enumerate(GATHER):
                arrived(sized(64, lanes), self.below[p][1])
                self.hand_over(p, -1)
                arrived(sized(64, lanes), self.above[p][0])
                self.hand_over(p, 1)

        def farthest(self):
            for p, (lanes, _) in enumerate(GATHER):
                arrived(sized(128, lanes), self.straight[p][2] if self.direct else self.relayed[p])
                self.hand_over(p, 2)

        def complete(self):
            arrived(g2.at[self.h, 0], self.across)

    expert = ep // 8
    column = lax.broadcasted_iota(jnp.int32, (1, 256), 1) + 256
    dense_own = jnp.logical_and(column >= 448, jnp.logical_or(core == 0, column >= 464))
    kinds = lax.broadcasted_iota(jnp.int32, (256, 128), 1)

    def hidden_unit(h, i, n):
        rows = slice(i * 256, (i + 1) * 256)
        x = [g2[h, c, rows, 0:HALF] for c in range(2)]
        info = g2[h, 0, rows, HALF:WIDE].astype(F32)
        factor = jnp.sum(jnp.where(kinds == expert, info, 0.0), axis=1, keepdims=True)
        if n == 1:
            mixed = info[:, 8:9] + info[:, 9:10]
            factor = jnp.where(column < 448, factor, jnp.where(dense_own, mixed, 0.0))

        def product(row):
            w = weights[row : row + 256, :]
            y = lax.dot_general(x[0], w[:, 0:HALF], NT, preferred_element_type=F32)
            return y + lax.dot_general(x[1], w[:, HALF:D], NT, preferred_element_type=F32)

        g = product(n * 256)
        u = product(HIDDEN + n * 256)
        hid[h, rows, n * 256 : (n + 1) * 256] = (g * jax.nn.sigmoid(g) * u * factor).astype(BF)

    halves = (pl.ds(0, 2), pl.ds(2, 2))

    def summand(ref, lanes, axis, where, half=None):
        at = [whole, whole, whole]
        at[axis] = where
        if half is not None:
            at[1 if axis == 0 else 0] = half
        return ref.at[at[0], at[1], at[2], :, pl.ds(lanes[0], lanes[1])]

    def cells(axis, index):
        for i in range(4):
            for j in range(4):
                at = [i, j]
                at.insert(axis, index)
                yield i, j, tuple(at)

    offsets = [(m, k) for m in (2, 1, -1, 0) for k in (2, 1, -1, 0) if (m, k) != (0, 0)]

    class Scatter:
        def __init__(self, h, direct):
            self.h, self.direct = h, direct
            self.swap = slots(2)
            self.far = None if direct else [slots(2) for p in parts]
            self.last = slots(3)
            self.nexts = slots(3)

        def down(self):
            h = self.h
            for whose, there in ((other, ps), (core, own_sum)):
                lanes = pl.ds(pl.multiple_of(whose * HALF, 128), HALF)
                for i in range(2):
                    x = hid[h, i * 256 : (i + 1) * 256, :]
                    y = jnp.dot(x, weights[2 * HIDDEN :, lanes], preferred_element_type=F32)
                    there[h, 2 * i : 2 * i + 2] = y.reshape(2, 4, 4, 8, HALF).astype(there.dtype)
                    if there is ps:
                        rows = pl.ds(2 * i, 2)
                        send(ps.at[h, rows], pin.at[h, rows], peer, csem, self.swap[i])

        def swapped(self):
            for i in range(2):
                arrived(pin.at[self.h, pl.ds(2 * i, 2)], self.swap[i])

        def joined(self, p, o):
            h = self.h
            lanes, (a, b, c) = SCATTER[p]
            cut = slice(lanes[0], lanes[0] + lanes[1])
            for i, j, at in cells(a, shifted(a, o)):
                at = (h,) + at + (slice(None), cut)
                tot[at] = (own_sum[at] + pin[at].astype(F32)).astype(BF)

        def open(self):
            h = self.h
            for p, (lanes, (a, b, c)) in enumerate(SCATTER):
                self.joined(p, 2)
                if self.direct:
                    self.whole_chunk(p, 2, 2)
                    continue
                for way, k in enumerate((1, -1)):
                    send(
                        summand(tot.at[h], lanes, a, shifted(a, 2), halves[way]),
                        rb.at[h, way, :, :, :, pl.ds(lanes[0], lanes[1])],
                        chip_at(a, k), csem, self.far[p][way],
                    )

        def whole_chunk(self, p, k, way):
            h = self.h
            lanes, (a, b, c) = SCATTER[p]
            send(
                summand(tot.at[h], lanes, a, shifted(a, k)), fin.at[h, way, :, :, :, pl.ds(lanes[0], lanes[1])],
                chip_at(a, k), csem, self.last[p],
            )

        def near(self, k):
            h = self.h
            way = 0 if k == 1 else 1
            half = halves[1 - way]
            for p, (lanes, (a, b, c)) in enumerate(SCATTER):
                self.joined(p, k)
                if self.direct:
                    self.whole_chunk(p, k, way)
                    continue
                send(
                    summand(tot.at[h], lanes, a, shifted(a, k), half),
                    fin.at[h, way, half, :, :, pl.ds(lanes[0], lanes[1])],
                    chip_at(a, k), csem, self.last[p],
                )

        def close(self):
            h = self.h
            for p, (lanes, (a, b, c)) in enumerate(SCATTER):
                cut = slice(lanes[0], lanes[0] + lanes[1])
                lanes_ds = pl.ds(lanes[0], lanes[1])
                for way, k in enumerate((1, -1)):
                    arrived(rb.at[h, way, :, :, :, lanes_ds], self.far[p][way])
                    for i, j, at in cells(a, shifted(a, k)):
                        if i // 2 == way:
                            at = (h,) + at + (slice(None), cut)
                            tot[at] = (tot[at].astype(F32) + rb[h, way, i % 2, j, :, cut].astype(F32)).astype(BF)
                    send(
                        summand(tot.at[h], lanes, a, shifted(a, k), halves[way]),
                        fin.at[h, way, halves[way], :, :, lanes_ds],
                        chip_at(a, k), csem, self.last[p],
                    )

        def own(self):
            for p in parts:
                self.joined(p, 0)

        def plane(self):
            h = self.h
            for p, (lanes, (a, b, c)) in enumerate(SCATTER):
                cut = slice(lanes[0], lanes[0] + lanes[1])
                lanes_ds = pl.ds(lanes[0], lanes[1])
                count = 3 if self.direct else 2
                arrived(fin.at[h, 0:count, :, :, :, lanes_ds], self.last[p])
                for i, j, at in cells(a, me[a]):
                    sum_ = tot[(h,) + at + (slice(None), cut)].astype(F32)
                    for n in range(count):
                        sum_ += fin[h, n, i, j, :, cut].astype(F32)
                    t1[h, i, j, :, cut] = sum_.astype(BF)
                d, e = [axis for axis in range(3) if axis != a]
                for n, (m, k) in enumerate(offsets):
                    send(
                        t1.at[h, shifted(d, m), shifted(e, k), :, lanes_ds], r2.at[h, n, :, lanes_ds],
                        chip_at(d, m, e, k), csem, self.nexts[p],
                    )

        def total(self):
            h = self.h
            for p, (lanes, (a, b, c)) in enumerate(SCATTER):
                cut = slice(lanes[0], lanes[0] + lanes[1])
                arrived(r2.at[h, :, :, pl.ds(lanes[0], lanes[1])], self.nexts[p])
                d, e = [axis for axis in range(3) if axis != a]
                sum_ = mid[h, :, cut] + t1[h, me[d], me[e], :, cut].astype(F32)
                for n in range(15):
                    sum_ += r2[h, n, :, cut].astype(F32)
                res[h, :, cut] = sum_.astype(BF)

    ga, gb = Gather(0, DIRECT[0]), Gather(1, DIRECT[1])
    sa, sb = Scatter(0, DIRECT[2]), Scatter(1, DIRECT[3])
    phase("attend_a")
    attend(0)
    attend(1)
    phase("project_a")
    base = pl.multiple_of(core * 48, 16)
    loads = (
        (eg_h, 0, 448), (dg_h.at[pl.ds(base, 64)], 448, 64),
        (eu_h, 512, 448), (du_h.at[pl.ds(base, 64)], 960, 64),
        (ed_h, 1024, 448), (dd_h.at[pl.ds(base, 64)], 1472, 64),
    )
    for src, row, count in loads:
        pltpu.make_async_copy(src, weights.at[pl.ds(row, count)], wsem).start()
    pltpu.make_async_copy(wo, wo, so).wait()
    project(0)
    pl.semaphore_wait(barrier, 37)
    pair(0)
    phase("attend_b1")
    attend(2)
    phase("norm_a")
    norm_half(0)
    ga.plane()
    phase("attend_b2")
    attend(3)
    phase("project_b")
    project(1)
    pair(1)
    wk_copy.wait()
    wv_copy.wait()
    nk[...] = jnp.dot(normed_all, wk[...], preferred_element_type=F32).astype(BF)
    nv[...] = jnp.dot(normed_all, wv[...], preferred_element_type=F32).astype(BF)
    phase("norm_b")
    norm_half(1)
    gb.plane()
    phase("rounds_a")
    ga.rounds()
    phase("relay_a")
    if not ga.direct:
        ga.relay(0)
    phase("rounds_b")
    gb.rounds()
    phase("relay_a2")
    if not ga.direct:
        for o in steps:
            ga.relay(o)
    ga.neighbours()
    phase("relay_b")
    if not gb.direct:
        for o in (0, *steps):
            gb.relay(o)
    phase("farthest_a")
    ga.farthest()
    pltpu.make_async_copy(weights, weights, wsem).wait()
    ga.complete()
    phase("hidden_a")
    hidden_unit(0, 0, 0)
    hidden_unit(0, 0, 1)
    phase("neighbours_b")
    gb.neighbours()
    phase("hidden_a2")
    hidden_unit(0, 1, 0)
    hidden_unit(0, 1, 1)
    phase("down_a")
    gb.farthest()
    sa.down()
    phase("complete_b")
    gb.complete()
    hidden_unit(1, 0, 0)
    phase("swap_a")
    sa.swapped()
    sa.open()
    sa.near(1)
    sa.near(-1)
    phase("hidden_b")
    hidden_unit(1, 0, 1)
    sa.own()
    hidden_unit(1, 1, 0)
    hidden_unit(1, 1, 1)
    phase("close_a")
    if not sa.direct:
        sa.close()
    phase("down_b")
    sb.down()
    phase("swap_b")
    sb.swapped()
    sb.open()
    sb.near(1)
    sb.near(-1)
    phase("plane_a")
    sa.plane()
    phase("close_b")
    if not sb.direct:
        sb.close()
    sb.own()
    phase("plane_b")
    sb.plane()
    phase("total_a")
    sa.total()
    phase("total_b")
    sb.total()
    phase("exchange")
    (slot,) = slots(1)
    send(res.at[other], got, peer, csem, slot)
    out[core] = res[core]
    arrived(got, slot)
    out[other] = got[...]
    phase("finish")
    assert used[0] == N_RECV, used[0]
    rows = gath.reshape(2048, WIDE).at[pl.ds(0, 2032)]
    pltpu.make_async_copy(rows, rows, gsem).wait()
    rows = ckv.reshape(2 * SEQS * CACHE, 128).at[pl.ds(0, 2040 * 8)]
    pltpu.make_async_copy(rows, rows, csem).wait()
    pltpu.make_async_copy(part, part, psem).wait()
    phase(None)


def finish_kernel(a, b, c, out, nk, nv):
    out[:, 0:HALF] = a[0]
    out[:, HALF:D] = a[1]
    nk[...] = b[...]
    nv[...] = c[...]


OUT_SHAPES = (
    jax.ShapeDtypeStruct((8, D), BF),
    jax.ShapeDtypeStruct((SEQS, 128), BF),
    jax.ShapeDtypeStruct((SEQS, 128), BF),
)


def layer(*args):
    return pl.pallas_call(
        layer_kernel,
        out_shape=(jax.ShapeDtypeStruct((2, 8, HALF), BF),) + OUT_SHAPES[1:],
        in_specs=[HB] * 20,
        out_specs=(VM, VM, VM),
        scratch_shapes=[
            pltpu.VMEM((2, 8, D), BF),
            pltpu.VMEM((1, D), F32),
            pltpu.VMEM((1, HEADS), F32),
            pltpu.SMEM((SEQS,), jnp.int32),
            pltpu.VMEM((1, D), F32),
            pltpu.VMEM((D,), BF),
            pltpu.VMEM((2, 8), jnp.int32),
            pltpu.VMEM((2, 8), BF),
            pltpu.SemaphoreType.DMA((8,)),
            pltpu.VMEM((D, 1024), BF),
            pltpu.VMEM((D, 128), BF),
            pltpu.VMEM((D, 128), BF),
            pltpu.VMEM((1024, D), BF),
            pltpu.VMEM((2, SEQS, CACHE, 128), BF),
            pltpu.VMEM((SEQS, HEADS, 128), F32),
            pltpu.VMEM((SEQS, 8, 128), F32),
            pltpu.VMEM((2, 8, D + 128), BF),
            pltpu.VMEM((2, 8, D + 128), BF),
            pltpu.VMEM((2, 8, HALF), F32),
            pltpu.VMEM((2, 2, 4, 4, 4, 8, WIDE), BF),
            pltpu.VMEM((3 * HIDDEN, D), BF),
            pltpu.VMEM((2, 512, HIDDEN), BF),
            pltpu.VMEM((2, 4, 4, 4, 8, HALF), BF),
            pltpu.VMEM((2, 4, 4, 4, 8, HALF), F32),
            pltpu.VMEM((2, 4, 4, 4, 8, HALF), BF),
            pltpu.VMEM((2, 4, 4, 4, 8, HALF), BF),
            pltpu.VMEM((2, 2, 2, 4, 8, HALF), BF),
            pltpu.VMEM((2, 3, 4, 4, 8, HALF), BF),
            pltpu.VMEM((2, 4, 4, 8, HALF), BF),
            pltpu.VMEM((2, 15, 8, HALF), BF),
            pltpu.VMEM((2, 8, HALF), BF),
            pltpu.VMEM((8, HALF), BF),
            pltpu.SemaphoreType.DMA((4,)),
            pltpu.SemaphoreType.DMA((4,)),
            pltpu.SemaphoreType.DMA,
            pltpu.SemaphoreType.DMA((2,)),
            pltpu.SemaphoreType.DMA,
            pltpu.SemaphoreType.DMA,
            pltpu.SemaphoreType.DMA,
            pltpu.SemaphoreType.DMA,
            pltpu.SemaphoreType.DMA((N_RECV,)),
        ],
        compiler_params=pltpu.CompilerParams(
            vmem_limit_bytes=67043328, collective_id=0, has_side_effects=True
        ),
        name="layer",
    )(*args)


def shards(
    tokens, norm_attn, w_query, w_key, w_value, w_out, attn_bias, cache_keys, cache_values, lengths,
    norm_ffn, expert_gate, expert_up, expert_down, dense_gate_w, dense_up_w, dense_down_w, dense_mix,
    routes, route_weights,
):
    results = layer(
        tokens.reshape(2, 8, D), norm_attn.reshape(1, D), attn_bias.reshape(1, HEADS), lengths,
        norm_ffn.reshape(1, D), dense_mix, routes.T, route_weights.T,
        w_query, w_key, w_value, w_out, cache_keys, cache_values,
        expert_gate.T, expert_up.T, expert_down, dense_gate_w.T, dense_up_w.T, dense_down_w,
    )
    return pl.pallas_call(
        finish_kernel, out_shape=OUT_SHAPES, in_specs=[VM] * 3, out_specs=(VM, VM, VM), name="finish"
    )(*results)


def solution(mesh):
    placed = (
        P("ep", None),
        P(),
        P(None, "tp"),
        P(None, "tp"),
        P(None, "tp"),
        P("tp", None),
        P("tp"),
        P("ep", None, "tp"),
        P("ep", None, "tp"),
        P("ep"),
        P(),
        P(None, ("ep", "tp")),
        P(None, ("ep", "tp")),
        P(("ep", "tp"), None),
        P(None, "ep"),
        P(None, "ep"),
        P("ep", None),
        P(),
        P(("ep", "tp"), None),
        P(("ep", "tp"), None),
    )
    return jax.shard_map(
        shards,
        mesh=mesh,
        in_specs=placed,
        out_specs=(P(("ep", "tp"), None), P("ep", "tp"), P("ep", "tp")),
        check_vma=False,
    )
```

```python
import functools
import jax
import jax.numpy as jnp
from jax import lax
from jax.experimental import pallas as pl
from jax.experimental.pallas import tpu as pltpu
from jax.sharding import PartitionSpec as P

D = 2048
BF = jnp.bfloat16
F32 = jnp.float32
EPSILON = 1e-06
SEQS = 16
CACHE = 1024
HEADS = 16
NT = (((1,), (1,)), ((), ()))
VM = pl.BlockSpec(memory_space=pltpu.VMEM)
HB = pl.BlockSpec(memory_space=pltpu.HBM)


def normed_rows(widened, gain):
    scale = lax.rsqrt(jnp.mean(widened * widened, axis=-1, keepdims=True) + EPSILON)
    return (widened * scale * gain).astype(BF)


def column_of(row, count):
    rows = lax.broadcasted_iota(jnp.int32, (count, count), 0)
    cols = lax.broadcasted_iota(jnp.int32, (count, count), 1)
    wide = jnp.broadcast_to(row, (count, count))
    return jnp.sum(jnp.where(rows == cols, wide, 0.0), axis=1, keepdims=True)


HALF = D // 2
WIDE = HALF + 128
MESH = pl.DeviceIdType.MESH
GATHER = (((0, 384), (2, 1, 0)), ((384, 384), (1, 0, 2)), ((768, 384), (0, 2, 1)))
SCATTER = (((0, 384), (0, 1, 2)), ((384, 384), (2, 0, 1)), ((768, 256), (1, 2, 0)))
HIDDEN = 512
GROUP = 4
N_RECV = 54
PHASE = [None]


def phase(name):
    if PHASE[0] is not None:
        PHASE[0].__exit__(None, None, None)
    PHASE[0] = jax.named_scope(name) if name else None
    if name:
        PHASE[0].__enter__()


def layer_kernel(
    tokens_h, norm_h, bias_h, lengths_h, gain_h, mix_h, routes_h, route_w_h,
    wq_h, wk_h, wv_h, wo_h, ck_h, cv_h, eg_h, eu_h, ed_h, dg_h, du_h, dd_h,
    out, nk, nv,
    tokens, norm, bias, lengths, gain, mix_w, routes, route_w, small,
    wq, wk, wv, wo, ckv, qs, xs, part,
    rx, mid, gath, weights, hid, ps, own_sum, pin, tot, fin, t1, r2, ex,
    sq, skv, so, sw, wsem, psem, gsem, csem, rsem,
):
    phase("start")
    ep = lax.axis_index("ep")
    core = lax.axis_index("tp")
    other = 1 - core
    me = (ep // 16, lax.rem(ep // 4, 4), lax.rem(ep, 4))
    strides = (16, 4, 1)

    def shifted(axis, k):
        return lax.rem(me[axis] + (k + 4), 4)

    def chip_at(axis, k, second=0, m=0):
        far = ep + (shifted(axis, k) - me[axis]) * strides[axis]
        return far + (shifted(second, m) - me[second]) * strides[second], core

    def q_copy(i):
        rows = pl.ds(i * 512, 512)
        return pltpu.make_async_copy(wq_h.at[rows], wq.at[rows], sq.at[i])

    def cache_start(i):
        rows = pl.ds(i * GROUP, GROUP)
        pltpu.make_async_copy(ck_h.at[rows], ckv.at[0, rows], skv.at[i]).start()
        pltpu.make_async_copy(cv_h.at[rows], ckv.at[1, rows], skv.at[i]).start()

    def cache_wait(i):
        both = ckv.at[:, pl.ds(i * GROUP, GROUP)]
        pltpu.make_async_copy(both, both, skv.at[i]).wait()

    ck, cv = ckv.at[0], ckv.at[1]
    wk_copy = pltpu.make_async_copy(wk_h, wk, sw.at[0])
    wv_copy = pltpu.make_async_copy(wv_h, wv, sw.at[1])
    def output_start():
        for i in range(16):
            row = (i % 8) * 128 + (i // 8) * 64
            pltpu.make_async_copy(wo_h.at[pl.ds(i * 64, 64)], wo.at[pl.ds(row, 64)], so).start()

    littles = [
        pltpu.make_async_copy(src, dst, small.at[n])
        for n, (src, dst) in enumerate((
            (tokens_h, tokens), (norm_h, norm), (routes_h, routes), (route_w_h, route_w),
            (bias_h, bias), (lengths_h, lengths), (gain_h, gain), (mix_h, mix_w),
        ))
    ]
    for copy in littles[:4]:
        copy.start()
    for i in range(4):
        q_copy(i).start()
    for copy in littles[4:]:
        copy.start()
    cache_start(0)
    peer = (ep, other)
    barrier = pltpu.get_barrier_semaphore()
    pl.semaphore_signal(barrier, inc=1, device_id=peer, device_id_type=MESH)
    for axis in range(3):
        for k in range(1, 4):
            target = chip_at(axis, k)
            pl.semaphore_signal(barrier, inc=1, device_id=target, device_id_type=MESH)
            pl.semaphore_signal(barrier, inc=1, device_id=(target[0], other), device_id_type=MESH)
            for m in range(1, 4):
                target = chip_at(axis, k, (axis + 1) % 3, m)
                pl.semaphore_signal(barrier, inc=1, device_id=target, device_id_type=MESH)
                pl.semaphore_signal(barrier, inc=1, device_id=(target[0], other), device_id_type=MESH)

    for copy in littles[:4]:
        copy.wait()

    kind = lax.broadcasted_iota(jnp.int32, (8, 128), 1)
    meta = jnp.zeros((8, 128), F32)
    for k in range(2):
        chosen = column_of(routes[k : k + 1, :].astype(F32), 8).astype(jnp.int32)
        share = column_of(route_w[k : k + 1, :].astype(F32), 8)
        meta += jnp.where(kind == chosen, share, 0.0)
    part[core, :, D : D + 128] = meta.astype(BF)
    part[other, :, D : D + 128] = jnp.zeros((8, 128), BF)

    normed_all = normed_rows(jnp.concatenate([tokens[0].astype(F32), tokens[1].astype(F32)], axis=0), norm[...])
    phase("query")
    query = jnp.zeros((SEQS, HEADS * 64), F32)
    for i in range(4):
        q_copy(i).wait()
        if i == 1:
            output_start()
        else:
            cache_start((1, 0, 2, 3)[i])
        query += jnp.dot(normed_all[:, i * 512 : (i + 1) * 512], wq[pl.ds(i * 512, 512), :], preferred_element_type=F32)
    wk_copy.start()
    wv_copy.start()
    query = query.astype(BF).astype(F32) * 0.125
    lane = lax.broadcasted_iota(jnp.int32, (SEQS, 128), 1)
    for i in range(8):
        pair = query[:, i * 128 : (i + 1) * 128]
        turned = pltpu.roll(pair, 64, 1)
        for j in range(2):
            h = 2 * i + j
            low = h < 8
            chosen = pair if (j == 0) == low else turned
            keep = (lane < 64) if low else (lane >= 64)
            qs[:, h, :] = jnp.where(keep, chosen, 0.0)

    phase("attend")
    for copy in littles[4:]:
        copy.wait()
    bias_col = column_of(bias[...], HEADS)
    tri = (
        lax.broadcasted_iota(jnp.int32, (256, 256), 0) > lax.broadcasted_iota(jnp.int32, (256, 256), 1)
    ).astype(BF)
    places = lax.broadcasted_iota(jnp.int32, (HEADS, CACHE), 1)
    lane8 = lax.broadcasted_iota(jnp.int32, (8, 128), 1)

    def attend(i):
        group = [i * GROUP + j for j in range(GROUP)]
        cache_wait(i)
        scores = [
            lax.dot_general(qs[b].astype(BF), ck[b], NT, preferred_element_type=F32) + bias_col for b in group
        ]
        takes, keeps, seen, stacked = [], [], [], []
        for b, z in zip(group, scores):
            visible = places < lengths[b]
            tail = jnp.log(1.0 + jnp.exp(-jnp.abs(z)))
            log_take = jnp.minimum(z, 0.0) - tail
            log_keep = jnp.where(visible, log_take - z, 0.0)
            high = log_keep.astype(BF)
            rest = (log_keep - high.astype(F32)).astype(BF)
            takes.append(log_take)
            keeps.append(log_keep)
            seen.append(visible)
            for n in range(4):
                stacked.append(high[:, n * 256 : (n + 1) * 256])
                stacked.append(rest[:, n * 256 : (n + 1) * 256])
        sums = jnp.dot(jnp.concatenate(stacked, axis=0), tri, preferred_element_type=F32)
        weights = []
        for at in range(GROUP):
            later = jnp.zeros((HEADS, 1), F32)
            after = [None] * 4
            for n in range(3, -1, -1):
                row = at * 128 + n * 32
                inner = sums[row : row + 16] + sums[row + 16 : row + 32]
                after[n] = inner + later
                later = later + inner[:, 0:1] + keeps[at][:, n * 256 : n * 256 + 1]
            after = jnp.concatenate(after, axis=1)
            weights.append(jnp.where(seen[at], jnp.exp(takes[at] + after), 0.0).astype(BF))
        for b, weight in zip(group, weights):
            mixed = jnp.dot(weight, cv[b], preferred_element_type=F32)
            xs[b] = jnp.where(lane8 < 64, mixed[0:8], mixed[8:16])

    def project(h):
        heads = jnp.concatenate([xs[h * 8 : (h + 1) * 8, r, :].astype(BF) for r in range(8)], axis=1)
        part[h, :, 0:D] = jnp.dot(heads, wo[...], preferred_element_type=F32).astype(BF)

    used = [0]

    def slots(count):
        used[0] += count
        return list(range(used[0] - count, used[0]))

    def send(src, dst, device, sem, slot):
        pltpu.make_async_remote_copy(
            src_ref=src, dst_ref=dst, send_sem=sem, recv_sem=rsem.at[slot], device_id=device, device_id_type=MESH
        ).start()

    def arrived(ref, slot):
        pltpu.make_async_remote_copy(
            src_ref=ref, dst_ref=ref, send_sem=csem, recv_sem=rsem.at[slot], device_id=peer, device_id_type=MESH
        ).wait_recv()

    pair_slots = slots(2)
    mix_row = mix_w[...].astype(F32).reshape(1, D)

    def pair(h):
        send(part.at[h], rx.at[h], peer, psem, pair_slots[h])

    def norm_half(h):
        arrived(rx.at[h], pair_slots[h])
        summed = part[h].astype(F32) + rx[h].astype(F32)
        middle = (tokens[h].astype(F32) + summed[:, 0:D]).astype(BF).astype(F32)
        normed = normed_rows(middle, gain[...]).astype(F32)
        mix = jax.nn.sigmoid(jnp.sum(normed * mix_row, axis=1, keepdims=True))
        mix_high = mix.astype(BF).astype(F32)
        meta = jnp.where(kind == 8, mix_high, summed[:, D : D + 128])
        meta = jnp.where(kind == 9, mix - mix_high, meta)
        mid[h] = middle
        own = jnp.where(core == 0, normed[:, 0:HALF], normed[:, HALF:D])
        gath[h, core, me[0], me[1], me[2], :, 0:HALF] = own.astype(BF)
        gath[h, core, me[0], me[1], me[2], :, HALF:WIDE] = meta.astype(BF)

    whole = pl.ds(0, 4)
    parts = range(3)
    steps = (1, -1, 2)
    g2 = gath.reshape(2, 2, 512, WIDE)

    def sized(rows):
        return g2.at[0, 0, pl.ds(0, rows)]

    class Gather:
        def __init__(self, h):
            self.h = h
            (self.first,) = slots(1)
            self.second = dict(zip(steps, slots(3)))
            (self.across,) = slots(1)
            self.straight = {o: dict(zip(steps, slots(3))) for o in (0, *steps)}

        def held(self, lanes, where):
            at = [me[0], me[1], me[2]]
            for axis, index in where.items():
                at[axis] = index
            return gath.at[self.h, core, at[0], at[1], at[2], :, pl.ds(lanes[0], lanes[1])]

        def spread(self, block, device, slot):
            send(block, block, device, gsem, slot)

        def plane(self):
            for m in (0, *steps):
                for k in (0, *steps):
                    for p, (lanes, (a, b, c)) in enumerate(GATHER):
                        if (k, m) != (0, 0):
                            slot = self.second[m] if m else self.first
                            self.spread(self.held(lanes, {}), chip_at(a, k, b, m), slot)

        def round(self, o):
            if o:
                arrived(sized(32), self.second[-o if o != 2 else 2])
            else:
                arrived(sized(24), self.first)
            for k in (2, 1, -1):
                for p, (lanes, (a, b, c)) in enumerate(GATHER):
                    block = self.held(lanes, {a: whole, b: shifted(b, o)})
                    self.spread(block, chip_at(c, k), self.straight[o][k])

        def rounds(self):
            for o in (0, *steps):
                self.round(o)
            for p in parts:
                self.hand_over(p, 0)

        def hand_over(self, p, o):
            lanes, (a, b, c) = GATHER[p]
            self.spread(self.held(lanes, {a: whole, b: whole, c: shifted(c, o)}), peer, self.across)

        def came(self, o):
            for k in (2, 1, -1):
                arrived(sized(32), self.straight[o][k])
                for lanes, (a, b, c) in GATHER:
                    block = self.held(lanes, {a: whole, b: shifted(b, o), c: shifted(c, -k if k != 2 else 2)})
                    self.spread(block, peer, self.across)

        def complete(self):
            arrived(g2.at[self.h, 0], self.across)

    expert = ep // 8
    column = lax.broadcasted_iota(jnp.int32, (1, 256), 1) + 256
    dense_own = jnp.logical_and(column >= 448, jnp.logical_or(core == 0, column >= 464))
    kinds = lax.broadcasted_iota(jnp.int32, (256, 128), 1)

    def hidden_unit(h, i, n):
        rows = slice(i * 256, (i + 1) * 256)
        x = [g2[h, c, rows, 0:HALF] for c in range(2)]
        info = g2[h, 0, rows, HALF:WIDE].astype(F32)
        factor = jnp.sum(jnp.where(kinds == expert, info, 0.0), axis=1, keepdims=True)
        if n == 1:
            mixed = info[:, 8:9] + info[:, 9:10]
            factor = jnp.where(column < 448, factor, jnp.where(dense_own, mixed, 0.0))

        def product(row):
            w = weights[row : row + 256, :]
            y = lax.dot_general(x[0], w[:, 0:HALF], NT, preferred_element_type=F32)
            return y + lax.dot_general(x[1], w[:, HALF:D], NT, preferred_element_type=F32)

        g = product(n * 256)
        u = product(HIDDEN + n * 256)
        hid[h, rows, n * 256 : (n + 1) * 256] = (g * jax.nn.sigmoid(g) * u * factor).astype(BF)


    def summand(ref, lanes, axis, where, half=None):
        at = [whole, whole, whole]
        at[axis] = where
        if half is not None:
            at[1 if axis == 0 else 0] = half
        return ref.at[at[0], at[1], at[2], :, pl.ds(lanes[0], lanes[1])]

    def cells(axis, index):
        for i in range(4):
            for j in range(4):
                at = [i, j]
                at.insert(axis, index)
                yield i, j, tuple(at)

    offsets = [(m, k) for m in (2, 1, -1, 0) for k in (2, 1, -1, 0) if (m, k) != (0, 0)]

    class Scatter:
        def __init__(self, h, swaps):
            self.h = h
            self.swap = slots(swaps)
            self.last = slots(3)
            self.nexts = slots(3)
            (self.cell,) = slots(1)

        def down(self, early):
            h = self.h
            if not early:
                quarter = HALF // 2
                for whose, there in ((other, ps), (core, own_sum)):
                    for n in range(2):
                        columns = pl.ds(pl.multiple_of(whose * HALF + n * quarter, 128), quarter)
                        cut = slice(n * quarter, (n + 1) * quarter)
                        for i in range(2):
                            x = hid[h, i * 256 : (i + 1) * 256, :]
                            y = jnp.dot(x, weights[2 * HIDDEN :, columns], preferred_element_type=F32)
                            y = y.reshape(2, 4, 4, 8, quarter).astype(there.dtype)
                            there[h, 2 * i : 2 * i + 2, :, :, :, cut] = y
                            if there is ps:
                                at = (pl.ds(2 * i, 2), whole, whole, slice(None), pl.ds(n * quarter, quarter))
                                send(ps.at[(h,) + at], pin.at[(h,) + at], peer, csem, self.swap[0])
                return
            for p, (lanes, _) in enumerate(SCATTER):
                cut = slice(lanes[0], lanes[0] + lanes[1])
                for whose, there in ((other, ps), (core, own_sum)):
                    columns = pl.ds(pl.multiple_of(whose * HALF + lanes[0], 128), lanes[1])
                    for i in range(2):
                        x = hid[h, i * 256 : (i + 1) * 256, :]
                        y = jnp.dot(x, weights[2 * HIDDEN :, columns], preferred_element_type=F32)
                        there[h, 2 * i : 2 * i + 2, :, :, :, cut] = y.reshape(2, 4, 4, 8, lanes[1]).astype(there.dtype)
                        if there is ps:
                            at = (pl.ds(2 * i, 2), whole, whole, slice(None), pl.ds(lanes[0], lanes[1]))
                            send(ps.at[(h,) + at], pin.at[(h,) + at], peer, csem, self.swap[p])
                if p:
                    self.chunks(p - 1)
            self.chunks(2)

        def joined(self, p, o):
            h = self.h
            lanes, (a, b, c) = SCATTER[p]
            cut = slice(lanes[0], lanes[0] + lanes[1])
            for i, j, at in cells(a, shifted(a, o)):
                at = (h,) + at + (slice(None), cut)
                tot[at] = (own_sum[at] + pin[at].astype(F32)).astype(BF)

        def chunks(self, p):
            lanes = SCATTER[p][0]
            if len(self.swap) > 1:
                arrived(pin.at[self.h, :, :, :, :, pl.ds(lanes[0], lanes[1])], self.swap[p])
            for k, way in ((2, 2), (1, 0), (-1, 1)):
                self.joined(p, k)
                self.whole_chunk(p, k, way)

        def whole_chunk(self, p, k, way):
            h = self.h
            lanes, (a, b, c) = SCATTER[p]
            send(
                summand(tot.at[h], lanes, a, shifted(a, k)), fin.at[h, way, :, :, :, pl.ds(lanes[0], lanes[1])],
                chip_at(a, k), csem, self.last[p],
            )

        def plane(self):
            h = self.h
            for p, (lanes, (a, b, c)) in enumerate(SCATTER):
                cut = slice(lanes[0], lanes[0] + lanes[1])
                lanes_ds = pl.ds(lanes[0], lanes[1])
                arrived(fin.at[h, :, :, :, :, lanes_ds], self.last[p])
                for i, j, at in cells(a, me[a]):
                    at = (h,) + at + (slice(None), cut)
                    sum_ = own_sum[at] + pin[at].astype(F32)
                    for n in range(3):
                        sum_ += fin[h, n, i, j, :, cut].astype(F32)
                    t1[h, i, j, :, cut] = sum_.astype(BF)
                d, e = [axis for axis in range(3) if axis != a]
                for n, (m, k) in enumerate(offsets):
                    send(
                        t1.at[h, shifted(d, m), shifted(e, k), :, lanes_ds], r2.at[core, n, :, lanes_ds],
                        (chip_at(d, m, e, k)[0], h), csem, self.nexts[p],
                    )

                @pl.when(core != h)
                def _():
                    send(t1.at[h, me[d], me[e], :, lanes_ds], ex.at[:, lanes_ds], peer, csem, self.cell)

        def total(self):
            h = self.h

            @pl.when(core == h)
            def _():
                arrived(ex, self.cell)
                for p, (lanes, (a, b, c)) in enumerate(SCATTER):
                    cut = slice(lanes[0], lanes[0] + lanes[1])
                    arrived(r2.at[:, :, :, pl.ds(lanes[0], lanes[1])], self.nexts[p])
                    d, e = [axis for axis in range(3) if axis != a]
                    for half in range(2):
                        there = slice(half * HALF + lanes[0], half * HALF + lanes[0] + lanes[1])
                        own = t1[h, me[d], me[e], :, cut] if half == h else ex[:, cut]
                        sum_ = mid[h, :, there] + own.astype(F32)
                        for n in range(15):
                            sum_ += r2[half, n, :, cut].astype(F32)
                        out[:, there] = sum_.astype(BF)

    ga, gb = Gather(0), Gather(1)
    sa, sb = Scatter(0, 1), Scatter(1, 3)
    phase("attend_a")
    attend(0)
    attend(1)
    phase("project_a")
    base = pl.multiple_of(core * 48, 16)
    loads = (
        (eg_h, 0, 448), (dg_h.at[pl.ds(base, 64)], 448, 64),
        (eu_h, 512, 448), (du_h.at[pl.ds(base, 64)], 960, 64),
        (ed_h, 1024, 448), (dd_h.at[pl.ds(base, 64)], 1472, 64),
    )
    for src, row, count in loads:
        pltpu.make_async_copy(src, weights.at[pl.ds(row, count)], wsem).start()
    pltpu.make_async_copy(wo, wo, so).wait()
    project(0)
    pl.semaphore_wait(barrier, 73)
    pair(0)
    phase("attend_b1")
    attend(2)
    phase("norm_a")
    norm_half(0)
    ga.plane()
    phase("attend_b2")
    attend(3)
    phase("project_b")
    project(1)
    pair(1)
    phase("norm_b")
    norm_half(1)
    gb.plane()
    phase("rounds_a")
    wk_copy.wait()
    wv_copy.wait()
    nk[...] = jnp.dot(normed_all, wk[...], preferred_element_type=F32).astype(BF)
    nv[...] = jnp.dot(normed_all, wv[...], preferred_element_type=F32).astype(BF)
    ga.rounds()
    phase("rounds_b")
    gb.rounds()
    phase("neighbours_a")
    for o in (0, 1, -1):
        ga.came(o)
    phase("farthest_a")
    ga.came(2)
    pltpu.make_async_copy(weights, weights, wsem).wait()
    ga.complete()
    phase("hidden_a")
    hidden_unit(0, 0, 0)
    hidden_unit(0, 0, 1)
    hidden_unit(0, 1, 0)
    phase("neighbours_b")
    for o in (0, 1, -1):
        gb.came(o)
    phase("hidden_a2")
    hidden_unit(0, 1, 1)
    gb.came(2)
    phase("down_a")
    sa.down(False)
    phase("complete_b")
    gb.complete()
    phase("hidden_b1")
    hidden_unit(1, 0, 0)
    phase("swap_a")
    arrived(pin.at[0], sa.swap[0])
    for p in parts:
        sa.chunks(p)
    phase("hidden_b")
    hidden_unit(1, 0, 1)
    hidden_unit(1, 1, 0)
    hidden_unit(1, 1, 1)
    phase("down_b")
    sb.down(True)
    phase("plane_a")
    sa.plane()
    phase("plane_b")
    sb.plane()
    phase("total_a")
    sa.total()
    phase("total_b")
    sb.total()
    phase("finish")
    assert used[0] == N_RECV, used[0]
    rows = gath.reshape(2048, WIDE).at[pl.ds(0, 2032)]
    pltpu.make_async_copy(rows, rows, gsem).wait()
    rows = ckv.reshape(2 * SEQS * CACHE, 128).at[pl.ds(0, 2040 * 8)]
    pltpu.make_async_copy(rows, rows, csem).wait()
    pltpu.make_async_copy(part, part, psem).wait()
    phase(None)


def finish_kernel(a, b, c, out, nk, nv):
    out[...] = a[...]
    nk[...] = b[...]
    nv[...] = c[...]


OUT_SHAPES = (
    jax.ShapeDtypeStruct((8, D), BF),
    jax.ShapeDtypeStruct((SEQS, 128), BF),
    jax.ShapeDtypeStruct((SEQS, 128), BF),
)


def layer(*args):
    return pl.pallas_call(
        layer_kernel,
        out_shape=OUT_SHAPES,
        in_specs=[HB] * 20,
        out_specs=(VM, VM, VM),
        scratch_shapes=[
            pltpu.VMEM((2, 8, D), BF),
            pltpu.VMEM((1, D), F32),
            pltpu.VMEM((1, HEADS), F32),
            pltpu.SMEM((SEQS,), jnp.int32),
            pltpu.VMEM((1, D), F32),
            pltpu.VMEM((D,), BF),
            pltpu.VMEM((2, 8), jnp.int32),
            pltpu.VMEM((2, 8), BF),
            pltpu.SemaphoreType.DMA((8,)),
            pltpu.VMEM((D, 1024), BF),
            pltpu.VMEM((D, 128), BF),
            pltpu.VMEM((D, 128), BF),
            pltpu.VMEM((1024, D), BF),
            pltpu.VMEM((2, SEQS, CACHE, 128), BF),
            pltpu.VMEM((SEQS, HEADS, 128), F32),
            pltpu.VMEM((SEQS, 8, 128), F32),
            pltpu.VMEM((2, 8, D + 128), BF),
            pltpu.VMEM((2, 8, D + 128), BF),
            pltpu.VMEM((2, 8, D), F32),
            pltpu.VMEM((2, 2, 4, 4, 4, 8, WIDE), BF),
            pltpu.VMEM((3 * HIDDEN, D), BF),
            pltpu.VMEM((2, 512, HIDDEN), BF),
            pltpu.VMEM((2, 4, 4, 4, 8, HALF), BF),
            pltpu.VMEM((2, 4, 4, 4, 8, HALF), F32),
            pltpu.VMEM((2, 4, 4, 4, 8, HALF), BF),
            pltpu.VMEM((2, 4, 4, 4, 8, HALF), BF),
            pltpu.VMEM((2, 3, 4, 4, 8, HALF), BF),
            pltpu.VMEM((2, 4, 4, 8, HALF), BF),
            pltpu.VMEM((2, 15, 8, HALF), BF),
            pltpu.VMEM((8, HALF), BF),
            pltpu.SemaphoreType.DMA((4,)),
            pltpu.SemaphoreType.DMA((4,)),
            pltpu.SemaphoreType.DMA,
            pltpu.SemaphoreType.DMA((2,)),
            pltpu.SemaphoreType.DMA,
            pltpu.SemaphoreType.DMA,
            pltpu.SemaphoreType.DMA,
            pltpu.SemaphoreType.DMA,
            pltpu.SemaphoreType.DMA((N_RECV,)),
        ],
        compiler_params=pltpu.CompilerParams(
            vmem_limit_bytes=67043328, collective_id=0, has_side_effects=True
        ),
        name="layer",
    )(*args)


def shards(
    tokens, norm_attn, w_query, w_key, w_value, w_out, attn_bias, cache_keys, cache_values, lengths,
    norm_ffn, expert_gate, expert_up, expert_down, dense_gate_w, dense_up_w, dense_down_w, dense_mix,
    routes, route_weights,
):
    results = layer(
        tokens.reshape(2, 8, D), norm_attn.reshape(1, D), attn_bias.reshape(1, HEADS), lengths,
        norm_ffn.reshape(1, D), dense_mix, routes.T, route_weights.T,
        w_query, w_key, w_value, w_out, cache_keys, cache_values,
        expert_gate.T, expert_up.T, expert_down, dense_gate_w.T, dense_up_w.T, dense_down_w,
    )
    return pl.pallas_call(
        finish_kernel, out_shape=OUT_SHAPES, in_specs=[VM] * 3, out_specs=(VM, VM, VM), name="finish"
    )(*results)


def solution(mesh):
    placed = (
        P("ep", None),
        P(),
        P(None, "tp"),
        P(None, "tp"),
        P(None, "tp"),
        P("tp", None),
        P("tp"),
        P("ep", None, "tp"),
        P("ep", None, "tp"),
        P("ep"),
        P(),
        P(None, ("ep", "tp")),
        P(None, ("ep", "tp")),
        P(("ep", "tp"), None),
        P(None, "ep"),
        P(None, "ep"),
        P("ep", None),
        P(),
        P(("ep", "tp"), None),
        P(("ep", "tp"), None),
    )
    return jax.shard_map(
        shards,
        mesh=mesh,
        in_specs=placed,
        out_specs=(P(("ep", "tp"), None), P("ep", "tp"), P("ep", "tp")),
        check_vma=False,
    )
```

```python
import functools
import jax
import jax.numpy as jnp
from jax import lax
from jax.experimental import pallas as pl
from jax.experimental.pallas import tpu as pltpu
from jax.sharding import PartitionSpec as P

D = 2048
BF = jnp.bfloat16
F32 = jnp.float32
EPSILON = 1e-06
SEQS = 16
CACHE = 1024
HEADS = 16
NT = (((1,), (1,)), ((), ()))
VM = pl.BlockSpec(memory_space=pltpu.VMEM)
HB = pl.BlockSpec(memory_space=pltpu.HBM)


def normed_rows(widened, gain):
    scale = lax.rsqrt(jnp.mean(widened * widened, axis=-1, keepdims=True) + EPSILON)
    return (widened * scale * gain).astype(BF)


def column_of(row, count):
    rows = lax.broadcasted_iota(jnp.int32, (count, count), 0)
    cols = lax.broadcasted_iota(jnp.int32, (count, count), 1)
    wide = jnp.broadcast_to(row, (count, count))
    return jnp.sum(jnp.where(rows == cols, wide, 0.0), axis=1, keepdims=True)


HALF = D // 2
WIDE = HALF + 128
MESH = pl.DeviceIdType.MESH
GATHER = (((0, 384), (2, 1, 0)), ((384, 384), (1, 0, 2)), ((768, 384), (0, 2, 1)))
SCATTER = (((0, 384), (0, 1, 2)), ((384, 384), (2, 0, 1)), ((768, 256), (1, 2, 0)))
HIDDEN = 512
GROUP = 4
N_RECV = 54
PHASE = [None]


def phase(name):
    if PHASE[0] is not None:
        PHASE[0].__exit__(None, None, None)
    PHASE[0] = jax.named_scope(name) if name else None
    if name:
        PHASE[0].__enter__()


def layer_kernel(
    tokens_h, norm_h, bias_h, lengths_h, gain_h, mix_h, routes_h, route_w_h,
    wq_h, wk_h, wv_h, wo_h, ck_h, cv_h, eg_h, eu_h, ed_h, dg_h, du_h, dd_h,
    out, nk, nv,
    tokens, norm, bias, lengths, gain, mix_w, routes, route_w, small,
    wq, wk, wv, wo, ckv, qs, xs, part,
    rx, mid, gath, weights, hid, acc, ps, own_sum, pin, tot, fin, t1, r2, ex,
    sq, skv, so, sw, wsem, psem, gsem, csem, rsem,
):
    phase("start")
    ep = lax.axis_index("ep")
    core = lax.axis_index("tp")
    other = 1 - core
    me = (ep // 16, lax.rem(ep // 4, 4), lax.rem(ep, 4))
    strides = (16, 4, 1)

    def shifted(axis, k):
        return lax.rem(me[axis] + (k + 4), 4)

    def chip_at(axis, k, second=0, m=0):
        far = ep + (shifted(axis, k) - me[axis]) * strides[axis]
        return far + (shifted(second, m) - me[second]) * strides[second], core

    def q_copy(i):
        rows = pl.ds(i * 512, 512)
        return pltpu.make_async_copy(wq_h.at[rows], wq.at[rows], sq.at[i])

    def cache_start(i):
        rows = pl.ds(i * GROUP, GROUP)
        pltpu.make_async_copy(ck_h.at[rows], ckv.at[0, rows], skv.at[i]).start()
        pltpu.make_async_copy(cv_h.at[rows], ckv.at[1, rows], skv.at[i]).start()

    def cache_wait(i):
        both = ckv.at[:, pl.ds(i * GROUP, GROUP)]
        pltpu.make_async_copy(both, both, skv.at[i]).wait()

    ck, cv = ckv.at[0], ckv.at[1]
    wk_copy = pltpu.make_async_copy(wk_h, wk, sw.at[0])
    wv_copy = pltpu.make_async_copy(wv_h, wv, sw.at[1])
    def output_start():
        for i in range(16):
            row = (i % 8) * 128 + (i // 8) * 64
            pltpu.make_async_copy(wo_h.at[pl.ds(i * 64, 64)], wo.at[pl.ds(row, 64)], so).start()

    littles = [
        pltpu.make_async_copy(src, dst, small.at[n])
        for n, (src, dst) in enumerate((
            (tokens_h, tokens), (norm_h, norm), (routes_h, routes), (route_w_h, route_w),
            (bias_h, bias), (lengths_h, lengths), (gain_h, gain), (mix_h, mix_w),
        ))
    ]
    for copy in littles[:4]:
        copy.start()
    for i in range(4):
        q_copy(i).start()
    for copy in littles[4:]:
        copy.start()
    cache_start(0)
    peer = (ep, other)
    barrier = pltpu.get_barrier_semaphore()
    pl.semaphore_signal(barrier, inc=1, device_id=peer, device_id_type=MESH)
    for axis in range(3):
        for k in range(1, 4):
            target = chip_at(axis, k)
            pl.semaphore_signal(barrier, inc=1, device_id=target, device_id_type=MESH)
            pl.semaphore_signal(barrier, inc=1, device_id=(target[0], other), device_id_type=MESH)
            for m in range(1, 4):
                target = chip_at(axis, k, (axis + 1) % 3, m)
                pl.semaphore_signal(barrier, inc=1, device_id=target, device_id_type=MESH)
                pl.semaphore_signal(barrier, inc=1, device_id=(target[0], other), device_id_type=MESH)

    for copy in littles[:4]:
        copy.wait()

    kind = lax.broadcasted_iota(jnp.int32, (8, 128), 1)
    meta = jnp.zeros((8, 128), F32)
    for k in range(2):
        chosen = column_of(routes[k : k + 1, :].astype(F32), 8).astype(jnp.int32)
        share = column_of(route_w[k : k + 1, :].astype(F32), 8)
        meta += jnp.where(kind == chosen, share, 0.0)
    part[core, :, D : D + 128] = meta.astype(BF)
    part[other, :, D : D + 128] = jnp.zeros((8, 128), BF)

    normed_all = normed_rows(jnp.concatenate([tokens[0].astype(F32), tokens[1].astype(F32)], axis=0), norm[...])
    phase("query")
    query = jnp.zeros((SEQS, HEADS * 64), F32)
    for i in range(4):
        q_copy(i).wait()
        if i == 0:
            cache_start(1)
        elif i == 1:
            output_start()
        query += jnp.dot(normed_all[:, i * 512 : (i + 1) * 512], wq[pl.ds(i * 512, 512), :], preferred_element_type=F32)
    query = query.astype(BF).astype(F32) * 0.125
    lane = lax.broadcasted_iota(jnp.int32, (SEQS, 128), 1)
    for i in range(8):
        pair = query[:, i * 128 : (i + 1) * 128]
        turned = pltpu.roll(pair, 64, 1)
        for j in range(2):
            h = 2 * i + j
            low = h < 8
            chosen = pair if (j == 0) == low else turned
            keep = (lane < 64) if low else (lane >= 64)
            qs[:, h, :] = jnp.where(keep, chosen, 0.0)

    phase("attend")
    for copy in littles[4:]:
        copy.wait()
    bias_col = column_of(bias[...], HEADS)
    tri = (
        lax.broadcasted_iota(jnp.int32, (256, 256), 0) > lax.broadcasted_iota(jnp.int32, (256, 256), 1)
    ).astype(BF)
    places = lax.broadcasted_iota(jnp.int32, (HEADS, CACHE), 1)
    lane8 = lax.broadcasted_iota(jnp.int32, (8, 128), 1)

    def attend(i):
        group = [i * GROUP + j for j in range(GROUP)]
        cache_wait(i)
        if i < 2:
            cache_start(i + 2)
        scores = [
            lax.dot_general(qs[b].astype(BF), ck[b], NT, preferred_element_type=F32) + bias_col for b in group
        ]
        takes, keeps, seen, stacked = [], [], [], []
        for b, z in zip(group, scores):
            visible = places < lengths[b]
            tail = jnp.log(1.0 + jnp.exp(-jnp.abs(z)))
            log_take = jnp.minimum(z, 0.0) - tail
            log_keep = jnp.where(visible, log_take - z, 0.0)
            high = log_keep.astype(BF)
            rest = (log_keep - high.astype(F32)).astype(BF)
            takes.append(log_take)
            keeps.append(log_keep)
            seen.append(visible)
            for n in range(4):
                stacked.append(high[:, n * 256 : (n + 1) * 256])
                stacked.append(rest[:, n * 256 : (n + 1) * 256])
        sums = jnp.dot(jnp.concatenate(stacked, axis=0), tri, preferred_element_type=F32)
        weights = []
        for at in range(GROUP):
            later = jnp.zeros((HEADS, 1), F32)
            after = [None] * 4
            for n in range(3, -1, -1):
                row = at * 128 + n * 32
                inner = sums[row : row + 16] + sums[row + 16 : row + 32]
                after[n] = inner + later
                later = later + inner[:, 0:1] + keeps[at][:, n * 256 : n * 256 + 1]
            after = jnp.concatenate(after, axis=1)
            weights.append(jnp.where(seen[at], jnp.exp(takes[at] + after), 0.0).astype(BF))
        for b, weight in zip(group, weights):
            mixed = jnp.dot(weight, cv[b], preferred_element_type=F32)
            xs[b] = jnp.where(lane8 < 64, mixed[0:8], mixed[8:16])

    def project(h):
        heads = jnp.concatenate([xs[h * 8 : (h + 1) * 8, r, :].astype(BF) for r in range(8)], axis=1)
        part[h, :, 0:D] = jnp.dot(heads, wo[...], preferred_element_type=F32).astype(BF)

    used = [0]

    def slots(count):
        used[0] += count
        return list(range(used[0] - count, used[0]))

    def send(src, dst, device, sem, slot):
        pltpu.make_async_remote_copy(
            src_ref=src, dst_ref=dst, send_sem=sem, recv_sem=rsem.at[slot], device_id=device, device_id_type=MESH
        ).start()

    def arrived(ref, slot):
        pltpu.make_async_remote_copy(
            src_ref=ref, dst_ref=ref, send_sem=csem, recv_sem=rsem.at[slot], device_id=peer, device_id_type=MESH
        ).wait_recv()

    pair_slots = slots(2)
    mix_row = mix_w[...].astype(F32).reshape(1, D)

    def pair(h):
        send(part.at[h], rx.at[h], peer, psem, pair_slots[h])

    def norm_half(h):
        arrived(rx.at[h], pair_slots[h])
        summed = part[h].astype(F32) + rx[h].astype(F32)
        middle = (tokens[h].astype(F32) + summed[:, 0:D]).astype(BF).astype(F32)
        normed = normed_rows(middle, gain[...]).astype(F32)
        mix = jax.nn.sigmoid(jnp.sum(normed * mix_row, axis=1, keepdims=True))
        mix_high = mix.astype(BF).astype(F32)
        meta = jnp.where(kind == 8, mix_high, summed[:, D : D + 128])
        meta = jnp.where(kind == 9, mix - mix_high, meta)
        mid[h] = middle
        own = jnp.where(core == 0, normed[:, 0:HALF], normed[:, HALF:D])
        gath[h, core, me[0], me[1], me[2], :, 0:HALF] = own.astype(BF)
        gath[h, core, me[0], me[1], me[2], :, HALF:WIDE] = meta.astype(BF)

    whole = pl.ds(0, 4)
    parts = range(3)
    steps = (1, -1, 2)
    g2 = gath.reshape(2, 2, 512, WIDE)

    def sized(rows):
        return g2.at[0, 0, pl.ds(0, rows)]

    class Gather:
        def __init__(self, h):
            self.h = h
            (self.first,) = slots(1)
            self.second = dict(zip(steps, slots(3)))
            (self.across,) = slots(1)
            self.straight = {o: dict(zip(steps, slots(3))) for o in (0, *steps)}

        def held(self, lanes, where):
            at = [me[0], me[1], me[2]]
            for axis, index in where.items():
                at[axis] = index
            return gath.at[self.h, core, at[0], at[1], at[2], :, pl.ds(lanes[0], lanes[1])]

        def spread(self, block, device, slot):
            send(block, block, device, gsem, slot)

        def plane(self):
            for m in (2, 1, -1, 0):
                for k in (2, 1, -1, 0):
                    for p, (lanes, (a, b, c)) in enumerate(GATHER):
                        if (k, m) != (0, 0):
                            slot = self.second[m] if m else self.first
                            self.spread(self.held(lanes, {}), chip_at(a, k, b, m), slot)

        def round(self, o):
            if o:
                arrived(sized(32), self.second[-o if o != 2 else 2])
            else:
                arrived(sized(24), self.first)
            for k in (2, 1, -1):
                for p, (lanes, (a, b, c)) in enumerate(GATHER):
                    block = self.held(lanes, {a: whole, b: shifted(b, o)})
                    self.spread(block, chip_at(c, k), self.straight[o][k])

        def rounds(self):
            for o in (2, 1, -1, 0):
                self.round(o)
            for p in parts:
                self.hand_over(p, 0)

        def hand_over(self, p, o):
            lanes, (a, b, c) = GATHER[p]
            self.spread(self.held(lanes, {a: whole, b: whole, c: shifted(c, o)}), peer, self.across)

        def came(self, o):
            for k in (2, 1, -1):
                arrived(sized(32), self.straight[o][k])
                for lanes, (a, b, c) in GATHER:
                    block = self.held(lanes, {a: whole, b: shifted(b, o), c: shifted(c, -k if k != 2 else 2)})
                    self.spread(block, peer, self.across)

        def complete(self):
            arrived(g2.at[self.h, 0], self.across)

    expert = ep // 8
    column = lax.broadcasted_iota(jnp.int32, (1, 256), 1) + 256
    dense_own = jnp.logical_and(column >= 448, jnp.logical_or(core == 0, column >= 464))
    kinds = lax.broadcasted_iota(jnp.int32, (256, 128), 1)

    def lane_product(h, whose, i, row):
        lanes = pl.ds(pl.multiple_of(whose * HALF, 128), HALF)
        x = g2[h, whose, i * 256 : (i + 1) * 256, 0:HALF]
        return lax.dot_general(x, weights[row : row + 256, lanes], NT, preferred_element_type=F32)

    def own_lanes(h):
        for i in range(2):
            for n in range(2):
                for kind_of in range(2):
                    acc[i, n, kind_of] = lane_product(h, core, i, kind_of * HIDDEN + n * 256)

    def hidden_unit(h, i, n, begun=False):
        rows = slice(i * 256, (i + 1) * 256)
        info = g2[h, 0, rows, HALF:WIDE].astype(F32)
        factor = jnp.sum(jnp.where(kinds == expert, info, 0.0), axis=1, keepdims=True)
        if n == 1:
            mixed = info[:, 8:9] + info[:, 9:10]
            factor = jnp.where(column < 448, factor, jnp.where(dense_own, mixed, 0.0))

        def product(row):
            x = [g2[h, c, rows, 0:HALF] for c in range(2)]
            w = weights[row : row + 256, :]
            y = lax.dot_general(x[0], w[:, 0:HALF], NT, preferred_element_type=F32)
            return y + lax.dot_general(x[1], w[:, HALF:D], NT, preferred_element_type=F32)

        if begun:
            g = acc[i, n, 0] + lane_product(h, other, i, n * 256)
            u = acc[i, n, 1] + lane_product(h, other, i, HIDDEN + n * 256)
        else:
            g = product(n * 256)
            u = product(HIDDEN + n * 256)
        hid[h, rows, n * 256 : (n + 1) * 256] = (g * jax.nn.sigmoid(g) * u * factor).astype(BF)


    def summand(ref, lanes, axis, where, half=None):
        at = [whole, whole, whole]
        at[axis] = where
        if half is not None:
            at[1 if axis == 0 else 0] = half
        return ref.at[at[0], at[1], at[2], :, pl.ds(lanes[0], lanes[1])]

    def cells(axis, index):
        for i in range(4):
            for j in range(4):
                at = [i, j]
                at.insert(axis, index)
                yield i, j, tuple(at)

    offsets = [(m, k) for m in (2, 1, -1, 0) for k in (2, 1, -1, 0) if (m, k) != (0, 0)]

    class Scatter:
        def __init__(self, h, swaps):
            self.h = h
            self.swap = slots(swaps)
            self.last = slots(3)
            self.nexts = slots(3)
            (self.cell,) = slots(1)

        def down(self, early):
            h = self.h
            if not early:
                quarter = HALF // 2
                for whose, there in ((other, ps), (core, own_sum)):
                    for n in range(2):
                        columns = pl.ds(pl.multiple_of(whose * HALF + n * quarter, 128), quarter)
                        cut = slice(n * quarter, (n + 1) * quarter)
                        y = jnp.dot(hid[h], weights[2 * HIDDEN :, columns], preferred_element_type=F32)
                        there[h, :, :, :, :, cut] = y.reshape(4, 4, 4, 8, quarter).astype(there.dtype)
                        if there is ps:
                            at = (h, whole, whole, whole, slice(None), pl.ds(n * quarter, quarter))
                            send(ps.at[at], pin.at[at], peer, csem, self.swap[0])
                return
            for p, (lanes, _) in enumerate(SCATTER):
                cut = slice(lanes[0], lanes[0] + lanes[1])
                for whose, there in ((other, ps), (core, own_sum)):
                    columns = pl.ds(pl.multiple_of(whose * HALF + lanes[0], 128), lanes[1])
                    y = jnp.dot(hid[h], weights[2 * HIDDEN :, columns], preferred_element_type=F32)
                    there[h, :, :, :, :, cut] = y.reshape(4, 4, 4, 8, lanes[1]).astype(there.dtype)
                    if there is ps:
                        at = (h, whole, whole, whole, slice(None), pl.ds(lanes[0], lanes[1]))
                        send(ps.at[at], pin.at[at], peer, csem, self.swap[p])
                if p:
                    self.chunks(p - 1)
            self.chunks(2)

        def joined(self, p, o):
            h = self.h
            lanes, (a, b, c) = SCATTER[p]
            cut = slice(lanes[0], lanes[0] + lanes[1])
            for i, j, at in cells(a, shifted(a, o)):
                at = (h,) + at + (slice(None), cut)
                tot[at] = (own_sum[at] + pin[at].astype(F32)).astype(BF)

        def chunks(self, p):
            lanes = SCATTER[p][0]
            if len(self.swap) > 1:
                arrived(pin.at[self.h, :, :, :, :, pl.ds(lanes[0], lanes[1])], self.swap[p])
            for k, way in ((2, 2), (1, 0), (-1, 1)):
                self.joined(p, k)
                self.whole_chunk(p, k, way)

        def whole_chunk(self, p, k, way):
            h = self.h
            lanes, (a, b, c) = SCATTER[p]
            send(
                summand(tot.at[h], lanes, a, shifted(a, k)), fin.at[h, way, :, :, :, pl.ds(lanes[0], lanes[1])],
                chip_at(a, k), csem, self.last[p],
            )

        def plane(self):
            h = self.h
            for p, (lanes, (a, b, c)) in enumerate(SCATTER):
                cut = slice(lanes[0], lanes[0] + lanes[1])
                lanes_ds = pl.ds(lanes[0], lanes[1])
                arrived(fin.at[h, :, :, :, :, lanes_ds], self.last[p])
                for i, j, at in cells(a, me[a]):
                    at = (h,) + at + (slice(None), cut)
                    sum_ = own_sum[at] + pin[at].astype(F32)
                    for n in range(3):
                        sum_ += fin[h, n, i, j, :, cut].astype(F32)
                    t1[h, i, j, :, cut] = sum_.astype(BF)
                d, e = [axis for axis in range(3) if axis != a]
                for n, (m, k) in enumerate(offsets):
                    send(
                        t1.at[h, shifted(d, m), shifted(e, k), :, lanes_ds], r2.at[core, n, :, lanes_ds],
                        (chip_at(d, m, e, k)[0], h), csem, self.nexts[p],
                    )

                @pl.when(core != h)
                def _():
                    send(t1.at[h, me[d], me[e], :, lanes_ds], ex.at[:, lanes_ds], peer, csem, self.cell)

        def total(self):
            h = self.h

            @pl.when(core == h)
            def _():
                arrived(ex, self.cell)
                for p, (lanes, (a, b, c)) in enumerate(SCATTER):
                    cut = slice(lanes[0], lanes[0] + lanes[1])
                    arrived(r2.at[:, :, :, pl.ds(lanes[0], lanes[1])], self.nexts[p])
                    d, e = [axis for axis in range(3) if axis != a]
                    for half in range(2):
                        there = slice(half * HALF + lanes[0], half * HALF + lanes[0] + lanes[1])
                        own = t1[h, me[d], me[e], :, cut] if half == h else ex[:, cut]
                        sum_ = mid[h, :, there] + own.astype(F32)
                        for n in range(15):
                            sum_ += r2[half, n, :, cut].astype(F32)
                        out[:, there] = sum_.astype(BF)

    ga, gb = Gather(0), Gather(1)
    sa, sb = Scatter(0, 1), Scatter(1, 3)
    phase("attend_a")
    attend(0)
    attend(1)
    phase("project_a")
    base = pl.multiple_of(core * 48, 16)
    loads = (
        (eg_h, 0, 448), (dg_h.at[pl.ds(base, 64)], 448, 64),
        (eu_h, 512, 448), (du_h.at[pl.ds(base, 64)], 960, 64),
        (ed_h, 1024, 448), (dd_h.at[pl.ds(base, 64)], 1472, 64),
    )
    for src, row, count in loads:
        pltpu.make_async_copy(src, weights.at[pl.ds(row, count)], wsem).start()
    wk_copy.start()
    wv_copy.start()
    pltpu.make_async_copy(wo, wo, so).wait()
    project(0)
    pl.semaphore_wait(barrier, 73)
    pair(0)
    phase("attend_b1")
    attend(2)
    phase("norm_a")
    norm_half(0)
    ga.plane()
    phase("attend_b2")
    attend(3)
    phase("project_b")
    project(1)
    pair(1)
    phase("norm_b")
    norm_half(1)
    gb.plane()
    phase("rounds_a")
    wk_copy.wait()
    wv_copy.wait()
    nk[...] = jnp.dot(normed_all, wk[...], preferred_element_type=F32).astype(BF)
    nv[...] = jnp.dot(normed_all, wv[...], preferred_element_type=F32).astype(BF)
    ga.rounds()
    phase("rounds_b")
    gb.rounds()
    phase("neighbours_a")
    for o in (2, 1, -1):
        ga.came(o)
    phase("farthest_a")
    ga.came(0)
    pltpu.make_async_copy(weights, weights, wsem).wait()
    phase("own_lanes")
    own_lanes(0)
    phase("complete_a")
    ga.complete()
    phase("hidden_a")
    hidden_unit(0, 0, 0, True)
    gb.came(2)
    hidden_unit(0, 0, 1, True)
    gb.came(1)
    hidden_unit(0, 1, 0, True)
    hidden_unit(0, 1, 1, True)
    phase("neighbours_b")
    gb.came(-1)
    gb.came(0)
    phase("down_a")
    sa.down(False)
    phase("complete_b")
    gb.complete()
    phase("hidden_b1")
    hidden_unit(1, 0, 0)
    phase("swap_a")
    arrived(pin.at[0], sa.swap[0])
    for p in parts:
        sa.chunks(p)
    phase("hidden_b")
    hidden_unit(1, 0, 1)
    hidden_unit(1, 1, 0)
    hidden_unit(1, 1, 1)
    phase("down_b")
    sb.down(True)
    phase("plane_a")
    sa.plane()
    phase("plane_b")
    sb.plane()
    phase("total_a")
    sa.total()
    phase("total_b")
    sb.total()
    phase("finish")
    assert used[0] == N_RECV, used[0]
    rows = gath.reshape(2048, WIDE).at[pl.ds(0, 2032)]
    pltpu.make_async_copy(rows, rows, gsem).wait()
    rows = ckv.reshape(2 * SEQS * CACHE, 128).at[pl.ds(0, 2040 * 8)]
    pltpu.make_async_copy(rows, rows, csem).wait()
    pltpu.make_async_copy(part, part, psem).wait()
    phase(None)


def finish_kernel(a, b, c, out, nk, nv):
    out[...] = a[...]
    nk[...] = b[...]
    nv[...] = c[...]


OUT_SHAPES = (
    jax.ShapeDtypeStruct((8, D), BF),
    jax.ShapeDtypeStruct((SEQS, 128), BF),
    jax.ShapeDtypeStruct((SEQS, 128), BF),
)


def layer(*args):
    return pl.pallas_call(
        layer_kernel,
        out_shape=OUT_SHAPES,
        in_specs=[HB] * 20,
        out_specs=(VM, VM, VM),
        scratch_shapes=[
            pltpu.VMEM((2, 8, D), BF),
            pltpu.VMEM((1, D), F32),
            pltpu.VMEM((1, HEADS), F32),
            pltpu.SMEM((SEQS,), jnp.int32),
            pltpu.VMEM((1, D), F32),
            pltpu.VMEM((D,), BF),
            pltpu.VMEM((2, 8), jnp.int32),
            pltpu.VMEM((2, 8), BF),
            pltpu.SemaphoreType.DMA((8,)),
            pltpu.VMEM((D, 1024), BF),
            pltpu.VMEM((D, 128), BF),
            pltpu.VMEM((D, 128), BF),
            pltpu.VMEM((1024, D), BF),
            pltpu.VMEM((2, SEQS, CACHE, 128), BF),
            pltpu.VMEM((SEQS, HEADS, 128), F32),
            pltpu.VMEM((SEQS, 8, 128), F32),
            pltpu.VMEM((2, 8, D + 128), BF),
            pltpu.VMEM((2, 8, D + 128), BF),
            pltpu.VMEM((2, 8, D), F32),
            pltpu.VMEM((2, 2, 4, 4, 4, 8, WIDE), BF),
            pltpu.VMEM((3 * HIDDEN, D), BF),
            pltpu.VMEM((2, 512, HIDDEN), BF),
            pltpu.VMEM((2, 2, 2, 256, 256), F32),
            pltpu.VMEM((2, 4, 4, 4, 8, HALF), BF),
            pltpu.VMEM((2, 4, 4, 4, 8, HALF), F32),
            pltpu.VMEM((2, 4, 4, 4, 8, HALF), BF),
            pltpu.VMEM((2, 4, 4, 4, 8, HALF), BF),
            pltpu.VMEM((2, 3, 4, 4, 8, HALF), BF),
            pltpu.VMEM((2, 4, 4, 8, HALF), BF),
            pltpu.VMEM((2, 15, 8, HALF), BF),
            pltpu.VMEM((8, HALF), BF),
            pltpu.SemaphoreType.DMA((4,)),
            pltpu.SemaphoreType.DMA((4,)),
            pltpu.SemaphoreType.DMA,
            pltpu.SemaphoreType.DMA((2,)),
            pltpu.SemaphoreType.DMA,
            pltpu.SemaphoreType.DMA,
            pltpu.SemaphoreType.DMA,
            pltpu.SemaphoreType.DMA,
            pltpu.SemaphoreType.DMA((N_RECV,)),
        ],
        compiler_params=pltpu.CompilerParams(
            vmem_limit_bytes=67043328, collective_id=0, has_side_effects=True
        ),
        name="layer",
    )(*args)


def shards(
    tokens, norm_attn, w_query, w_key, w_value, w_out, attn_bias, cache_keys, cache_values, lengths,
    norm_ffn, expert_gate, expert_up, expert_down, dense_gate_w, dense_up_w, dense_down_w, dense_mix,
    routes, route_weights,
):
    results = layer(
        tokens.reshape(2, 8, D), norm_attn.reshape(1, D), attn_bias.reshape(1, HEADS), lengths,
        norm_ffn.reshape(1, D), dense_mix, routes.T, route_weights.T,
        w_query, w_key, w_value, w_out, cache_keys, cache_values,
        expert_gate.T, expert_up.T, expert_down, dense_gate_w.T, dense_up_w.T, dense_down_w,
    )
    return pl.pallas_call(
        finish_kernel, out_shape=OUT_SHAPES, in_specs=[VM] * 3, out_specs=(VM, VM, VM), name="finish"
    )(*results)


def solution(mesh):
    placed = (
        P("ep", None),
        P(),
        P(None, "tp"),
        P(None, "tp"),
        P(None, "tp"),
        P("tp", None),
        P("tp"),
        P("ep", None, "tp"),
        P("ep", None, "tp"),
        P("ep"),
        P(),
        P(None, ("ep", "tp")),
        P(None, ("ep", "tp")),
        P(("ep", "tp"), None),
        P(None, "ep"),
        P(None, "ep"),
        P("ep", None),
        P(),
        P(("ep", "tp"), None),
        P(("ep", "tp"), None),
    )
    return jax.shard_map(
        shards,
        mesh=mesh,
        in_specs=placed,
        out_specs=(P(("ep", "tp"), None), P("ep", "tp"), P("ep", "tp")),
        check_vma=False,
    )
```
